32 devices in a mesh: rep: 2 (over y), fs: 4 (over z), tp: 4 (over x, core).
Axes of the slice: x: 2, y: 2, z: 4, core: 2. Of those that a mesh axis runs over, the one named last changes fastest.
Arguments:
- tokens: bfloat16 [8, 512, 2048], P(('rep', 'fs')), may hold values from -6 to 6
- first_gain: float32 [2048], replicated, may hold values from 0.1 to 1.9
- in_matrix: float32 [2048, 2048], P('fs', 'tp'), may hold values from -0.125 to 0.125
- in_scale: float32 [2048], P('tp'), may hold values from 0.5 to 2
- conv_taps: float32 [4, 2048], P(None, 'tp'), may hold values from -3 to 3
- decay_rate: float32 [2, 2048], P(None, 'tp'), may hold values from 0 to 1, as said below
- recall_maps: float32 [2, 8, 256, 256], P(None, 'tp'), may hold values from -0.375 to 0.375
- admit_maps: float32 [2, 8, 256, 256], P(None, 'tp'), may hold values from -0.375 to 0.375
- out_matrix: float32 [2048, 2048], P('fs', 'tp'), may hold values from -0.125 to 0.125
- out_scale: float32 [2048], P('fs'), may hold values from 0.5 to 2
- second_gain: float32 [2048], replicated, may hold values from 0.1 to 1.9
- up_matrix: float32 [2048, 4096], P('fs', 'tp'), may hold values from -0.125 to 0.125
- up_scale: float32 [4096], P('tp'), may hold values from 0.5 to 2
- down_matrix: float32 [2048, 4096], P('fs', 'tp'), may hold values from -0.09375 to 0.09375
- down_scale: float32 [2048], P('fs'), may hold values from 0.5 to 2
Outputs:
- layer_out: bfloat16 [8, 512, 2048], P(('rep', 'fs'))
The draws below stay inside these ranges and needn't reach their ends.
Inputs may be any that keep to these rules, and one draw needn't show every extreme that they name: `decay_rate`: positive per-step decay rates.
All inputs are finite; a program needn't handle non-finite values.
Results may differ from the reference program's by a relative error of at most 0.024.
Values may be sent and summed in bfloat16 or wider, within the bound.
A program may use at most 64 MiB of HBM per device.

```python
import math
import jax
import jax.numpy as jnp
from jax import lax

D = 2048
BLOCK = 256
BLOCKS = 8
FF = 4096
TAPS = 4
LEN = 512
REC_WIDTH = 2048
SEQS = 8
N_TP = 4


def draw_decay_rate(key, part):
    pick_key, slow_key, fast_key = jax.random.split(jax.random.fold_in(key, 17), 3)
    shape = (2, REC_WIDTH)
    slow_share = 0.5
    slow_pick = jax.random.bernoulli(pick_key, slow_share, shape)
    slow_rate = jnp.exp(jax.random.uniform(slow_key, shape, jnp.float32, math.log(0.05), math.log(0.5))) / LEN
    fast_rate = jnp.exp(jax.random.uniform(fast_key, shape, jnp.float32, math.log(0.005), math.log(0.02)))
    return jnp.where(slow_pick, slow_rate, fast_rate).astype(jnp.float32)


def level_of(key, extent, cuts, least, top_value):
    factor_of, own = 1.0, jax.random.fold_in(key, 6)
    for dim, blocks in cuts:
        heights = jnp.exp(jax.random.uniform(jax.random.fold_in(own, dim), (blocks,), jnp.float32, least / len(cuts), top_value / len(cuts)))
        factor_of = factor_of * jnp.repeat(heights, extent[dim] // blocks).reshape([-1 if axis == dim else 1 for axis in range(len(extent))])
    return factor_of


def bell_draw(rng, dims, deviation, reach, pieces=(), dtype=jnp.bfloat16):
    level = level_of(rng, dims, pieces, -0.22, 0.18) if pieces else 1.0
    entries = jax.random.normal(rng, dims, jnp.float32) * deviation * level
    return jnp.minimum(jnp.maximum(entries, -reach), reach).astype(dtype)


def setup_inputs(seed: int = 0) -> dict:
    seeds = jax.random.split(jax.random.key(seed), 16)
    return {
        "tokens": bell_draw(seeds[0], (SEQS, LEN, D), 1.0, 6.0, ((0, 8),)),
        "first_gain": jnp.clip(1.0 + 0.18 * jax.random.normal(seeds[1], (D,), jnp.float32), 0.1, 1.9),
        "in_matrix": bell_draw(seeds[2], (D, REC_WIDTH), D ** -0.5, 0.125, ((0, 4), (1, 4)), jnp.float32),
        "in_scale": jnp.clip(jnp.exp(math.log(2.0) - 1.3862944 * jax.random.uniform(seeds[3], (REC_WIDTH,), jnp.float32) ** level_of(seeds[3], (REC_WIDTH,), ((0, 4),), -0.2, 0.2)), 0.5, 2.0),
        "conv_taps": bell_draw(seeds[4], (TAPS, REC_WIDTH), TAPS ** -0.5, 3.0, ((1, 4),), jnp.float32),
        "decay_rate": draw_decay_rate(jax.random.fold_in(seeds[15], 71), 0),
        "recall_maps": bell_draw(seeds[6], (2, BLOCKS, BLOCK, BLOCK), BLOCK ** -0.5, 0.375, ((1, 4),), jnp.float32),
        "admit_maps": bell_draw(seeds[7], (2, BLOCKS, BLOCK, BLOCK), BLOCK ** -0.5, 0.375, ((1, 4),), jnp.float32),
        "out_matrix": bell_draw(seeds[8], (D, REC_WIDTH), REC_WIDTH ** -0.5, 0.125, ((0, 4), (1, 4)), jnp.float32),
        "out_scale": jnp.clip(jnp.exp(math.log(2.0) - 1.3862944 * jax.random.uniform(seeds[9], (D,), jnp.float32) ** level_of(seeds[9], (D,), ((0, 4),), -0.2, 0.2)), 0.5, 2.0),
        "second_gain": jnp.clip(1.0 + 0.18 * jax.random.normal(seeds[10], (D,), jnp.float32), 0.1, 1.9),
        "up_matrix": bell_draw(seeds[11], (D, FF), D ** -0.5, 0.125, ((0, 4), (1, 4)), jnp.float32),
        "up_scale": jnp.clip(jnp.exp(math.log(2.0) - 1.3862944 * jax.random.uniform(seeds[12], (FF,), jnp.float32) ** level_of(seeds[12], (FF,), ((0, 4),), -0.2, 0.2)), 0.5, 2.0),
        "down_matrix": bell_draw(seeds[13], (D, FF), FF ** -0.5, 0.09375, ((0, 4), (1, 4)), jnp.float32),
        "down_scale": jnp.clip(jnp.exp(math.log(2.0) - 1.3862944 * jax.random.uniform(seeds[14], (D,), jnp.float32) ** level_of(seeds[14], (D,), ((0, 4),), -0.2, 0.2)), 0.5, 2.0),
    }


EPSILON = 1e-06
RATE_GAIN = 8.0

def normalize(stream, gain):
    return stream * lax.rsqrt(lax.optimization_barrier(jnp.mean(stream * stream, axis=-1, keepdims=True)) + EPSILON) * gain

def convolve(values, taps):
    length = values.shape[0]
    count = taps.shape[0]
    padded = jnp.pad(values, ((count // 2, count - 1 - count // 2), (0, 0)))
    total = taps[0] * padded[0:length]
    for offset in range(1, count):
        total = total + taps[offset] * padded[offset:offset + length]
    return total

def block_map(values, maps):
    length = values.shape[0]
    count, width = (maps.shape[0], maps.shape[1])
    grouped = values.reshape(length, count, width)
    mapped = jnp.einsum('lnj,njk->lnk', grouped, maps, precision=lax.Precision.HIGHEST)
    return mapped.reshape(length, count * width)

def combine_steps(earlier, later):
    return (earlier[0] * later[0], later[0] * earlier[1] + later[1])

def one_direction(values, rate, recall_map, admit_map):
    recall = jax.nn.sigmoid(block_map(values, recall_map))
    admit = jax.nn.sigmoid(block_map(values, admit_map))
    log_decay = -RATE_GAIN * recall * rate
    decay = jnp.exp(log_decay)
    drive = jnp.sqrt(-jnp.expm1(2.0 * log_decay)) * admit * values
    carried = lax.associative_scan(combine_steps, (decay, drive), axis=0)
    return carried[1]

def recurrence(values, rates, recall_maps, admit_maps):
    forward = one_direction(values, rates[0], recall_maps[0], admit_maps[0])
    backward = one_direction(values[::-1], rates[1], recall_maps[1], admit_maps[1])[::-1]
    return forward + backward

def block_sum(values, matrix):
    length, width = values.shape
    model = matrix.shape[0]
    split_values = values.astype(jnp.float32).reshape(length, N_TP, width // N_TP)
    split_matrix = matrix.astype(jnp.float32).reshape(model, N_TP, width // N_TP)
    parts = jnp.einsum('lte,dte->tld', split_values, split_matrix, precision=lax.Precision.HIGHEST)
    rounded = lax.optimization_barrier(parts.astype(jnp.bfloat16))
    return lax.optimization_barrier(jnp.sum(rounded.astype(jnp.float32), axis=0))

def reference(tokens, first_gain, in_matrix, in_scale, conv_taps, decay_rate, recall_maps, admit_maps, out_matrix, out_scale, second_gain, up_matrix, up_scale, down_matrix, down_scale):
    in_cols = in_matrix.astype(jnp.bfloat16)
    out_rows = out_matrix.astype(jnp.bfloat16)
    up_cols = up_matrix.astype(jnp.bfloat16)
    down_rows = down_matrix.astype(jnp.bfloat16)
    in_factor = in_scale.astype(jnp.bfloat16)
    out_factor = out_scale.astype(jnp.bfloat16)
    up_factor = up_scale.astype(jnp.bfloat16)
    down_factor = down_scale.astype(jnp.bfloat16)

    def one_sequence(sequence):
        stream = sequence.astype(jnp.float32)
        normed = normalize(stream, first_gain).astype(jnp.bfloat16)
        before = (jnp.dot(normed, in_cols, preferred_element_type=jnp.float32) * in_factor).astype(jnp.bfloat16)
        conv_out = convolve(before.astype(jnp.float32), conv_taps)
        mixed = recurrence(conv_out, decay_rate, recall_maps, admit_maps).astype(jnp.bfloat16)
        middle = stream + out_factor * block_sum(mixed, out_rows)
        second_normed = normalize(middle, second_gain).astype(jnp.bfloat16)
        raised = jnp.dot(second_normed, up_cols, preferred_element_type=jnp.float32) * up_factor
        active = jnp.square(jax.nn.relu(raised)).astype(jnp.bfloat16)
        return (middle + down_factor * block_sum(active, down_rows)).astype(jnp.bfloat16)
    return lax.map(one_sequence, tokens)
```

```python
import functools
import jax
import jax.numpy as jnp
from jax import lax
from jax.experimental import pallas as pl
from jax.experimental.pallas import tpu as pltpu
from jax.sharding import PartitionSpec as P

EPSILON = 1e-06
RATE_GAIN = 8.0
LANES = 128
SEGMENTS = 8
PAD = 8


def normalize(stream, gain):
    return stream * lax.rsqrt(jnp.mean(stream * stream, axis=-1, keepdims=True) + EPSILON) * gain


def one_minus_exp(y):
    series = 1.0 + y * (1.0 / 6.0)
    for k in (5.0, 4.0, 3.0, 2.0):
        series = 1.0 + y * (1.0 / k) * series
    return jnp.where(y > -0.25, -y * series, 1.0 - jnp.exp(y))


def sigmoid(x):
    return 0.5 * jnp.tanh(0.5 * x) + 0.5


def gate_part(padded, taps_ref, rate_ref, recall_ref, admit_ref, decay, drive, length, serve=None):
    directions, groups, block, _ = recall_ref.shape
    taps = taps_ref.shape[0]
    rows = length // SEGMENTS

    def tile_step(tile, _):
        base = pl.multiple_of(tile * rows, rows)
        conv = jnp.zeros((rows, padded.shape[1]), jnp.float32)
        window = padded[pl.ds(base, rows + 2 * PAD), :]
        for k in range(taps):
            first = PAD - taps // 2 + k
            conv = conv + taps_ref[k : k + 1, :] * window[first : first + rows, :]
        narrow = conv.astype(jnp.bfloat16)
        for g in range(groups):
            values = conv[:, g * block : (g + 1) * block]
            left = narrow[:, g * block : (g + 1) * block]
            for d in range(directions):
                recall = sigmoid(jnp.dot(left, recall_ref[d, g].astype(jnp.bfloat16), preferred_element_type=jnp.float32))
                admit = sigmoid(jnp.dot(left, admit_ref[d, g].astype(jnp.bfloat16), preferred_element_type=jnp.float32))
                log_decay = recall * (-RATE_GAIN * rate_ref[d : d + 1, g * block : (g + 1) * block])
                a = jnp.exp(log_decay)
                b = jnp.sqrt(one_minus_exp(2.0 * log_decay)) * admit * values
                for c in range(block // LANES):
                    where = g * (block // LANES) + c
                    decay[d, where, pl.ds(base, rows), :] = a[:, c * LANES : (c + 1) * LANES]
                    drive[d, where, pl.ds(base, rows), :] = b[:, c * LANES : (c + 1) * LANES]
        return 0

    if serve is None:
        lax.fori_loop(0, SEGMENTS, tile_step, 0)
        return
    for first in range(0, SEGMENTS, 2):
        lax.fori_loop(first, first + 2, tile_step, 0)
        serve()


def scan_part(decay, drive, prefix, mixed_ref, length, serve=None):
    directions, chunks = decay.shape[:2]
    steps = length // SEGMENTS
    lanes = [(d, c) for d in range(directions) for c in range(chunks)]

    def scan_step(s, carried):
        out = []
        for (d, c), (state, product) in zip(lanes, carried):
            at = s if d == 0 else steps - 1 - s
            a = decay[d, c, pl.ds(at, SEGMENTS, stride=steps), :]
            b = drive[d, c, pl.ds(at, SEGMENTS, stride=steps), :]
            state = a * state + b
            product = a * product
            drive[d, c, pl.ds(at, SEGMENTS, stride=steps), :] = state
            prefix[d, c, pl.ds(at, SEGMENTS, stride=steps), :] = product
            out.append((state, product))
        return tuple(out)

    start = tuple((jnp.zeros((SEGMENTS, LANES), jnp.float32), jnp.ones((SEGMENTS, LANES), jnp.float32)) for _ in lanes)
    if serve is None:
        ends = lax.fori_loop(0, steps, scan_step, start, unroll=4)
    else:
        ends = start
        for first in range(0, steps, steps // 4):
            ends = lax.fori_loop(first, first + steps // 4, scan_step, ends, unroll=4)
            serve()
    ends = dict(zip(lanes, ends))

    for c in range(chunks):
        carries = []
        for d in range(directions):
            state, product = ends[(d, c)]
            order = range(SEGMENTS) if d == 0 else range(SEGMENTS - 1, -1, -1)
            carry = jnp.zeros((1, LANES), jnp.float32)
            entering = {}
            for k in order:
                entering[k] = carry
                carry = product[k : k + 1, :] * carry + state[k : k + 1, :]
            carries.append(entering)
        for k in range(SEGMENTS):
            span = pl.ds(k * steps, steps)
            total = drive[0, c, span, :] + prefix[0, c, span, :] * carries[0][k]
            total = total + (drive[1, c, span, :] + prefix[1, c, span, :] * carries[1][k])
            mixed_ref[span, c * LANES : (c + 1) * LANES] = total.astype(jnp.bfloat16)
        if serve is not None:
            serve()


def recurrence_kernel(before_ref, taps_ref, rate_ref, recall_ref, admit_ref, mixed_ref, padded, decay, drive, prefix):
    length, width = before_ref.shape
    edge = jnp.zeros((PAD, width), jnp.float32)
    padded[pl.ds(0, PAD), :] = edge
    padded[pl.ds(PAD + length, PAD), :] = edge
    padded[pl.ds(PAD, length), :] = before_ref[...].astype(jnp.float32)
    gate_part(padded, taps_ref, rate_ref, recall_ref, admit_ref, decay, drive, length)
    scan_part(decay, drive, prefix, mixed_ref, length)


def recurrence(before, taps, rates, recall_maps, admit_maps):
    length, width = before.shape
    directions = rates.shape[0]
    chunks = width // LANES
    plane = pltpu.VMEM((directions, chunks, length, LANES), jnp.float32)
    return pl.pallas_call(
        recurrence_kernel,
        out_shape=jax.ShapeDtypeStruct((length, width), jnp.bfloat16),
        in_specs=[pl.BlockSpec(memory_space=pltpu.VMEM)] * 5,
        out_specs=pl.BlockSpec(memory_space=pltpu.VMEM),
        scratch_shapes=[pltpu.VMEM((length + 2 * PAD, width), jnp.float32), plane, plane, plane],
        compiler_params=pltpu.CompilerParams(vmem_limit_bytes=24 * 2**20),
        cost_estimate=pl.CostEstimate(flops=16 * length * width * 256, bytes_accessed=8 * 2**20, transcendentals=8 * length * width),
        name="recurrence",
    )(before, taps, rates, recall_maps, admit_maps)


def contract_last(left, right):
    return lax.dot_general(
        left, right, (((1,), (1,)), ((), ())), preferred_element_type=jnp.float32
    )


def gather(shard):
    copies = lax.axis_size("rep")
    if shard.shape[0] % (16 * copies):
        return lax.all_gather(shard.astype(jnp.bfloat16), "fs", axis=0, tiled=True)
    rows = shard.shape[0] // copies
    part = lax.dynamic_slice_in_dim(shard, lax.axis_index("rep") * rows, rows, 0)
    return lax.all_gather(part.astype(jnp.bfloat16), ("fs", "rep"), axis=0, tiled=True)


def body(
    tokens,
    first_gain,
    in_matrix,
    in_scale,
    conv_taps,
    decay_rate,
    recall_maps,
    admit_maps,
    out_matrix,
    out_scale,
    second_gain,
    up_matrix,
    up_scale,
    down_matrix,
    down_scale,
):
    stream = tokens.reshape(tokens.shape[1], tokens.shape[2]).astype(jnp.float32)
    factors = lax.all_gather(
        jnp.stack([out_scale, down_scale]).astype(jnp.bfloat16), "fs", axis=1, tiled=True
    )
    in_cols = gather(in_matrix)
    normed = normalize(stream, first_gain).astype(jnp.bfloat16)
    before = (
        jnp.dot(normed, in_cols, preferred_element_type=jnp.float32) * in_scale.astype(jnp.bfloat16)
    ).astype(jnp.bfloat16)
    mixed = recurrence(before, conv_taps, decay_rate, recall_maps, admit_maps)
    partial_value = contract_last(mixed, gather(out_matrix))
    middle = stream + factors[0] * lax.psum(partial_value.astype(jnp.bfloat16), "tp").astype(
        jnp.float32
    )
    second_normed = normalize(middle, second_gain).astype(jnp.bfloat16)
    raised = jnp.dot(second_normed, gather(up_matrix), preferred_element_type=jnp.float32)
    active = jnp.square(jax.nn.relu(raised * up_scale.astype(jnp.bfloat16))).astype(jnp.bfloat16)
    lowered = contract_last(active, gather(down_matrix))
    result = (
        middle + factors[1] * lax.psum(lowered.astype(jnp.bfloat16), "tp").astype(jnp.float32)
    ).astype(jnp.bfloat16)
    return result.reshape(tokens.shape)

MESH = pl.DeviceIdType.MESH
UNITS = 12
AHEAD = 2
EDGE_SERVES = ((), (), (), (), (), (0, 1, 12, 13, 24, 2, 14, 25, 3,), (15,), (), (), (26,), (), (), (4,), (), (16,), (), (27,), (), (), (), (5, 17,), (), (), (), (), (), (28,), (), (), (6,), (), (), (18,), (29,), (7,), (19,), (30,), (8,), (20,), (31,), (), (9,), (), (21,), (), (), (32,), (), (), (10,), (), (22, 33, 11, 23,), (), (), (34,), (), (), (35,), (), (), (), (), (), (), (), (), (), (), ())
INNER_SERVES = ((), (), (), (), (), (0, 12, 1, 13, 2, 24, 3, 14, 4, 25, 5, 15, 6, 26, 7, 16, 8, 27, 9, 17, 10, 28,), (11, 18,), (), (), (29,), (), (), (19,), (), (30,), (), (20,), (), (), (), (31, 21, 32,), (), (22,), (), (), (), (33,), (), (), (), (), (23,), (34,), (35,), (), (), (), (), (), (), (), (), (), (), (), (), (), (), (), (), (), (), (), (), (), (), (), (), (), (), (), (), (), (), (), (), (), (), ())


def layer_kernel(
    names, tokens_hbm, first_ref, in_hbm, in_scale_ref, taps_ref, rate_ref, recall_hbm, admit_hbm,
    out_hbm, out_scale_ref, second_ref, up_hbm, up_scale_ref, down_hbm, down_scale_ref,
    result_ref,
    tokens, in_own, out_own, up_own, down_own, recall_ref, admit_ref,
    in_all, out_all, up_all, down_all, scales_all, normed, second_normed, padded, decay, drive, prefix, mixed, active,
    parts, near_parts, pairs, far_pairs, middle, load, send, recv,
):
    replica, place, rank = (lax.axis_index(name) for name in names)
    rep_name, fs_name, tp_name = names
    fs = 4
    length, model = tokens.shape
    block = model // fs
    half, quarter = block // 2, block // 4
    mate = place + 1 - 2 * lax.rem(place, 2)
    inner = lax.rem(lax.div(place + 1, 2), 2)
    other = fs - 1 - place
    other_mate = fs - 1 - mate
    slots = (mate, inner * other + (1 - inner) * other_mate, inner * other_mate + (1 - inner) * other)
    core = lax.rem(rank, 2)
    near = rank + 1 - 2 * core
    far = lax.rem(rank + 2, 4)
    sends, recvs = [0], [0]

    def fresh(counter):
        counter[0] += 1
        return counter[0] - 1

    def copy(src, dst, axis, peer, into=None):
        index = fresh(recvs) if into is None else into
        return pltpu.make_async_remote_copy(
            src_ref=src, dst_ref=dst, send_sem=send.at[fresh(sends)], recv_sem=recv.at[index],
            device_id={axis: peer}, device_id_type=MESH,
        )

    started, inner_started = [], []

    def start(*copies):
        for one in copies:
            one.start()
            started.append(one)

    loads = [
        pltpu.make_async_copy(src, dst, load.at[i])
        for i, (src, dst) in enumerate((
            (in_hbm, in_own), (out_hbm, out_own), (tokens_hbm, tokens), (up_hbm, up_own), (down_hbm, down_own),
            (recall_hbm, recall_ref), (admit_hbm, admit_ref),
        ))
    ]
    for one in loads:
        one.start()
    load_in, load_out, load_tokens, load_up, load_down, load_recall, load_admit = loads

    barrier = pltpu.get_barrier_semaphore()
    greeted = [(rep_name, 1 - replica)]
    greeted += [(fs_name, lax.rem(place + k, fs)) for k in range(1, fs)]
    greeted += [(tp_name, near), (tp_name, far)]
    for axis, peer in greeted:
        pl.semaphore_signal(barrier, inc=1, device_id={axis: peer}, device_id_type=MESH)

    own_rows = pl.ds(pl.multiple_of(place * block, block), block)
    load_in.wait()
    in_all[own_rows, :] = in_own[...].astype(jnp.bfloat16)
    load_out.wait()
    out_all[own_rows, :] = out_own[...].astype(jnp.bfloat16)
    scales_all[place, 0:1, :] = out_scale_ref[...]
    scales_all[place, 1:2, :] = down_scale_ref[...]

    wide = up_all.shape[1] // 2

    def view(owner, unit):
        def rows(step):
            return pl.ds(pl.multiple_of(owner * block + replica * half + step * quarter, quarter), quarter)

        if unit < 4:
            return (in_all, out_all)[unit // 2].at[rows(unit % 2), :]
        if unit < 8:
            return up_all.at[rows(unit % 2), (unit - 4) // 2 * wide : ((unit - 4) // 2 + 1) * wide]
        return down_all.at[rows((unit - 8) // 2), unit % 2 * wide : (unit % 2 + 1) * wide]

    to_mate, to_other, pass_mate, pass_other, pass_last, swaps = [], [], [], [], [], []
    for unit in range(UNITS):
        into = [fresh(recvs) for _ in range(3)]
        own, first, second, third = (view(owner, unit) for owner in (place,) + slots)
        to_mate.append(copy(own, own, fs_name, mate, into[0]))
        to_other.append(copy(own, own, fs_name, other, into[1]))
        pass_mate.append(copy(first, first, fs_name, other, into[2]))
        pass_other.append(copy(second, second, fs_name, mate, into[1]))
        pass_last.append(copy(third, third, fs_name, mate, into[2]))
        swaps.append([copy(part, part, rep_name, 1 - replica) for part in (first, second, third)])
    arrivals = (to_mate, to_other, pass_last)
    sent = {"mate": 0, "other": 0}

    def start_inner(one):
        one.start()
        inner_started.append(one)

    def serve_edge(codes):
        for code in codes:
            slot, unit = code // UNITS, code % UNITS
            arrivals[slot][unit].wait_recv()
            swaps[unit][slot].start()

    def serve_inner(codes):
        for code in codes:
            slot, unit = code // UNITS, code % UNITS
            arrivals[slot][unit].wait_recv()
            swaps[unit][slot].start()
            if slot == 0:
                start_inner(pass_mate[unit])
                if sent["other"] < UNITS:
                    start_inner(to_other[sent["other"]])
                    sent["other"] += 1
            elif slot == 1:
                start_inner(pass_other[unit])
            else:
                start_inner(pass_last[unit])
                if sent["mate"] < UNITS:
                    to_mate[sent["mate"]].start()
                    sent["mate"] += 1

    point = [0]

    def serve():
        edge_codes, inner_codes = EDGE_SERVES[point[0]], INNER_SERVES[point[0]]
        point[0] += 1
        if edge_codes:
            pl.when(inner == 0)(lambda: serve_edge(edge_codes))
        if inner_codes:
            pl.when(inner == 1)(lambda: serve_inner(inner_codes))

    def need_weights(*units):
        serve()
        for slot in range(3):
            for unit in units:
                swaps[unit][slot].wait_recv()

    pl.semaphore_wait(barrier, len(greeted))

    @pl.when(inner == 0)
    def _():
        for unit in range(4):
            to_mate[unit].start()

    @pl.when(inner == 1)
    def _():
        for unit in range(AHEAD):
            to_mate[unit].start()
            start_inner(to_other[unit])
        sent["mate"] = sent["other"] = AHEAD

    scale_copies = [
        copy(scales_all.at[place], scales_all.at[place], fs_name, lax.rem(place + k, fs)) for k in range(1, fs)
    ]
    start(*scale_copies)
    load_up.wait()
    up_all[own_rows, :] = up_own[...].astype(jnp.bfloat16)
    load_down.wait()
    down_all[own_rows, :] = down_own[...].astype(jnp.bfloat16)

    @pl.when(inner == 0)
    def _():
        for unit in range(4, UNITS):
            to_mate[unit].start()

    load_tokens.wait()
    serve()
    tile = 64
    for i in range(4):

        def norm_step(k, _, i=i):
            at = pl.ds(pl.multiple_of((2 * i + k) * tile, tile), tile)
            normed[at, :] = normalize(tokens[at, :].astype(jnp.float32), first_ref[...]).astype(jnp.bfloat16)
            return 0

        lax.fori_loop(0, length // tile // 4, norm_step, 0)
        serve()

    edge = jnp.zeros((PAD, padded.shape[1]), jnp.float32)
    padded[pl.ds(0, PAD), :] = edge
    padded[pl.ds(PAD + length, PAD), :] = edge
    load_recall.wait()
    load_admit.wait()
    need_weights(0, 1)
    step = 256
    for i in range(in_all.shape[1] // step):
        at = slice(i * step, (i + 1) * step)
        product = jnp.dot(normed[...], in_all[:, at], preferred_element_type=jnp.float32)
        product = product * in_scale_ref[:, at].astype(jnp.bfloat16).astype(jnp.float32)
        padded[pl.ds(PAD, length), at] = product.astype(jnp.bfloat16).astype(jnp.float32)
        serve()
    gate_part(padded, taps_ref, rate_ref, recall_ref, admit_ref, decay, drive, length, serve)
    scan_part(decay, drive, prefix, mixed, length, serve)

    need_weights(2, 3)
    for one in scale_copies:
        one.wait_recv()
    chunks = model // step
    kept = pl.ds(pl.multiple_of(core * (length // 2), length // 2), length // 2)
    given = pl.ds(pl.multiple_of((1 - core) * (length // 2), length // 2), length // 2)

    class Combine:
        def __init__(self, stage):
            self.stage = stage
            self.to_near = [
                copy(parts.at[stage, k, given, :], near_parts.at[stage, k], tp_name, near) for k in range(chunks)
            ]
            self.to_far = [copy(pairs.at[stage, k], far_pairs.at[stage, k], tp_name, far) for k in range(chunks)]

        def put(self, k, partial):
            parts[self.stage, k] = partial.astype(jnp.bfloat16)
            start(self.to_near[k])

        def pair(self, k):
            self.to_near[k].wait_recv()
            total = parts[self.stage, k, kept, :].astype(jnp.float32) + near_parts[self.stage, k].astype(jnp.float32)
            pairs[self.stage, k] = total.astype(jnp.bfloat16)
            start(self.to_far[k])

        def total(self, k):
            self.to_far[k].wait_recv()
            return pairs[self.stage, k].astype(jnp.float32) + far_pairs[self.stage, k].astype(jnp.float32)

    def factor(owner, which, at):
        return scales_all[owner, which : which + 1, at].astype(jnp.bfloat16).astype(jnp.float32)

    one_stage = Combine(0)
    for k in range(chunks + 2):
        if k < chunks:
            one_stage.put(k, contract_last(mixed[...], out_all[k * step : (k + 1) * step, :]))
        serve()
        if k >= 2:
            one_stage.pair(k - 2)
    squares = jnp.zeros((length // 2, 1), jnp.float32)
    for k in range(chunks):
        serve()
        at = slice(k * step, (k + 1) * step)
        inside = slice(k * step % block, k * step % block + step)
        value = tokens[kept, at].astype(jnp.float32) + factor(k * step // block, 0, inside) * one_stage.total(k)
        middle[:, at] = value
        squares = squares + jnp.sum(value * value, axis=1, keepdims=True)
    inverse = lax.rsqrt(squares * (1.0 / model) + EPSILON)
    spreads = []
    for i in range(2):
        rows = slice(i * (length // 4), (i + 1) * (length // 4))
        at = pl.ds(pl.multiple_of(core * (length // 2) + i * (length // 4), length // 4), length // 4)
        second_normed[at, :] = (middle[rows, :] * inverse[rows, :] * second_ref[...]).astype(jnp.bfloat16)
        spreads.append(copy(second_normed.at[at, :], second_normed.at[at, :], tp_name, near))
        start(spreads[i])
    serve()
    for one in spreads:
        one.wait_recv()

    for part in range(2):
        need_weights(4 + 2 * part, 5 + 2 * part)
        for i in range(part * (wide // step), (part + 1) * (wide // step)):
            at = slice(i * step, (i + 1) * step)
            raised = jnp.dot(second_normed[...], up_all[:, at], preferred_element_type=jnp.float32)
            raised = raised * up_scale_ref[:, at].astype(jnp.bfloat16).astype(jnp.float32)
            active[:, at] = jnp.square(jnp.maximum(raised, 0.0)).astype(jnp.bfloat16)
            serve()

    two_stage = Combine(1)
    order = [(place, 0, None), (place, 1, None)] + [(slots[j], q, j) for q in range(2) for j in range(3)]
    finals = []

    def finish(k):
        owner, q, _ = order[k]
        total = two_stage.total(k)
        for h in range(2):
            inside = slice(h * half + q * quarter, h * half + (q + 1) * quarter)
            at = pl.ds(pl.multiple_of(owner * block + h * half + q * quarter, quarter), quarter)
            value = middle[:, at] + factor(owner, 1, inside) * total[:, h * quarter : (h + 1) * quarter]
            result_ref[kept, at] = value.astype(jnp.bfloat16)
            finals.append(copy(result_ref.at[kept, at], result_ref.at[kept, at], tp_name, near))
            start(finals[-1])

    for k in range(chunks + 4):
        if k < chunks:
            owner, q, j = order[k]
            if j is not None:
                serve()
                for unit in (8 + 2 * q, 9 + 2 * q):
                    swaps[unit][j].wait_recv()
            rows = [
                down_all[pl.ds(pl.multiple_of(owner * block + h * half + q * quarter, quarter), quarter), :] for h in range(2)
            ]
            two_stage.put(k, contract_last(active[...], jnp.concatenate(rows, axis=0)))
        if 1 <= k <= chunks:
            serve()
            two_stage.pair(k - 1)
        if k >= 4:
            serve()
            finish(k - 4)
    serve()
    for one in finals:
        one.wait_recv()
    for one in started:
        one.wait_send()
    for unit in range(UNITS):
        to_mate[unit].wait_send()
        for one in swaps[unit]:
            one.wait_send()

    @pl.when(inner == 1)
    def _():
        for one in inner_started:
            one.wait_send()


def fused_body(
    tokens, first_gain, in_matrix, in_scale, conv_taps, decay_rate, recall_maps, admit_maps,
    out_matrix, out_scale, second_gain, up_matrix, up_scale, down_matrix, down_scale,
):
    length, model = tokens.shape[1:]
    width, hidden = in_matrix.shape[1], up_matrix.shape[1]
    fs = lax.axis_size("fs")
    block, step = model // fs, 256
    directions = decay_rate.shape[0]
    plane = pltpu.VMEM((directions, width // LANES, length, LANES), jnp.float32)
    gate = pltpu.VMEM(recall_maps.shape, jnp.float32)
    pieces = pltpu.VMEM((2, model // step, length // 2, step), jnp.bfloat16)
    vmem, hbm = pl.BlockSpec(memory_space=pltpu.VMEM), pl.BlockSpec(memory_space=pl.ANY)
    arrived = UNITS * 6 + 3 + 2 * 2 * (model // step) + 2 + 2 * (model // step)
    result = pl.pallas_call(
        functools.partial(layer_kernel, ("rep", "fs", "tp")),
        out_shape=jax.ShapeDtypeStruct((length, model), jnp.bfloat16),
        in_specs=[hbm, vmem, hbm, vmem, vmem, vmem, hbm, hbm, hbm, vmem, vmem, hbm, vmem, hbm, vmem],
        out_specs=vmem,
        scratch_shapes=[
            pltpu.VMEM((length, model), jnp.bfloat16),
            pltpu.VMEM((block, width), jnp.float32),
            pltpu.VMEM((block, width), jnp.float32),
            pltpu.VMEM((block, hidden), jnp.float32),
            pltpu.VMEM((block, hidden), jnp.float32),
            gate, gate,
            pltpu.VMEM((model, width), jnp.bfloat16),
            pltpu.VMEM((model, width), jnp.bfloat16),
            pltpu.VMEM((model, hidden), jnp.bfloat16),
            pltpu.VMEM((model, hidden), jnp.bfloat16),
            pltpu.VMEM((fs, 2, block), jnp.float32),
            pltpu.VMEM((length, model), jnp.bfloat16),
            pltpu.VMEM((length, model), jnp.bfloat16),
            pltpu.VMEM((length + 2 * PAD, width), jnp.float32),
            plane, plane, plane,
            pltpu.VMEM((length, width), jnp.bfloat16),
            pltpu.VMEM((length, hidden), jnp.bfloat16),
            pltpu.VMEM((2, model // step, length, step), jnp.bfloat16),
            pieces, pieces, pieces,
            pltpu.VMEM((length // 2, model), jnp.float32),
            pltpu.SemaphoreType.DMA((7,)),
            pltpu.SemaphoreType.DMA((arrived + 2 * UNITS,)),
            pltpu.SemaphoreType.DMA((arrived,)),
        ],
        compiler_params=pltpu.CompilerParams(
            collective_id=0, has_side_effects=True, vmem_limit_bytes=61 * 2**20
        ),
        name="layer",
    )(
        tokens.reshape(length, model), first_gain[None], in_matrix, in_scale[None], conv_taps, decay_rate,
        recall_maps, admit_maps, out_matrix, out_scale[None], second_gain[None], up_matrix, up_scale[None], down_matrix,
        down_scale[None],
    )
    return result.reshape(tokens.shape)


def solution(mesh):
    placed = (
        P(("rep", "fs"), None, None),
        P(),
        P("fs", "tp"),
        P("tp"),
        P(None, "tp"),
        P(None, "tp"),
        P(None, "tp", None, None),
        P(None, "tp", None, None),
        P("fs", "tp"),
        P("fs"),
        P(),
        P("fs", "tp"),
        P("tp"),
        P("fs", "tp"),
        P("fs"),
    )
    small = (mesh.shape["rep"], mesh.shape["fs"], mesh.shape["tp"]) == (2, 4, 4)
    return jax.shard_map(
        fused_body if small else body, mesh=mesh, in_specs=placed, out_specs=P(("rep", "fs"), None, None), check_vma=False
    )
```

```python
import functools
import jax
import jax.numpy as jnp
from jax import lax
from jax.experimental import pallas as pl
from jax.experimental.pallas import tpu as pltpu
from jax.sharding import PartitionSpec as P

EPSILON = 1e-06
RATE_GAIN = 8.0
LANES = 128
SEGMENTS = 8
PAD = 8
GAP = 8


def normalize(stream, gain):
    return stream * lax.rsqrt(jnp.mean(stream * stream, axis=-1, keepdims=True) + EPSILON) * gain


def one_minus_exp(y):
    series = 1.0 + y * (1.0 / 6.0)
    for k in (5.0, 4.0, 3.0, 2.0):
        series = 1.0 + y * (1.0 / k) * series
    return jnp.where(y > -0.25, -y * series, 1.0 - jnp.exp(y))


def sigmoid(x):
    return 0.5 * jnp.tanh(0.5 * x) + 0.5


def gate_part(padded, taps_ref, rate_ref, recall_ref, admit_ref, decay, drive, length, serve=None):
    directions, groups, block, _ = recall_ref.shape
    taps = taps_ref.shape[0]
    rows = length // SEGMENTS
    pitch = decay.shape[2] // SEGMENTS

    def tile_step(tile, _):
        base = pl.multiple_of(tile * rows, rows)
        into = pl.multiple_of(tile * pitch, 8)
        conv = jnp.zeros((rows, padded.shape[1]), jnp.float32)
        window = padded[pl.ds(base, rows + 2 * PAD), :]
        for k in range(taps):
            first = PAD - taps // 2 + k
            conv = conv + taps_ref[k : k + 1, :] * window[first : first + rows, :]
        narrow = conv.astype(jnp.bfloat16)
        for g in range(groups):
            values = conv[:, g * block : (g + 1) * block]
            left = narrow[:, g * block : (g + 1) * block]
            for d in range(directions):
                recall = sigmoid(jnp.dot(left, recall_ref[d, g].astype(jnp.bfloat16), preferred_element_type=jnp.float32))
                admit = sigmoid(jnp.dot(left, admit_ref[d, g].astype(jnp.bfloat16), preferred_element_type=jnp.float32))
                log_decay = recall * (-RATE_GAIN * rate_ref[d : d + 1, g * block : (g + 1) * block])
                a = jnp.exp(log_decay)
                b = jnp.sqrt(one_minus_exp(2.0 * log_decay)) * admit * values
                for c in range(block // LANES):
                    where = g * (block // LANES) + c
                    decay[d, where, pl.ds(into, rows), :] = a[:, c * LANES : (c + 1) * LANES]
                    drive[d, where, pl.ds(into, rows), :] = b[:, c * LANES : (c + 1) * LANES]
        return 0

    if serve is None:
        lax.fori_loop(0, SEGMENTS, tile_step, 0)
        return
    for first in range(0, SEGMENTS, 2):
        lax.fori_loop(first, first + 2, tile_step, 0)
        serve()


def scan_part(decay, drive, prefix, mixed_ref, length, serve=None):
    directions, chunks = decay.shape[:2]
    steps = length // SEGMENTS
    pitch = decay.shape[2] // SEGMENTS
    lanes = [(d, c) for d in range(directions) for c in range(chunks)]

    def scan_step(s, carried):
        out = []
        for (d, c), (state, product) in zip(lanes, carried):
            at = s if d == 0 else steps - 1 - s
            a = decay[d, c, pl.ds(at, SEGMENTS, stride=pitch), :]
            b = drive[d, c, pl.ds(at, SEGMENTS, stride=pitch), :]
            state = a * state + b
            product = a * product
            drive[d, c, pl.ds(at, SEGMENTS, stride=pitch), :] = state
            prefix[d, c, pl.ds(at, SEGMENTS, stride=pitch), :] = product
            out.append((state, product))
        return tuple(out)

    start = tuple((jnp.zeros((SEGMENTS, LANES), jnp.float32), jnp.ones((SEGMENTS, LANES), jnp.float32)) for _ in lanes)
    if serve is None:
        ends = lax.fori_loop(0, steps, scan_step, start, unroll=4)
    else:
        ends = start
        for first in range(0, steps, steps // 4):
            ends = lax.fori_loop(first, first + steps // 4, scan_step, ends, unroll=4)
            serve()
    ends = dict(zip(lanes, ends))

    for c in range(chunks):
        carries = []
        for d in range(directions):
            state, product = ends[(d, c)]
            order = range(SEGMENTS) if d == 0 else range(SEGMENTS - 1, -1, -1)
            carry = jnp.zeros((1, LANES), jnp.float32)
            entering = {}
            for k in order:
                entering[k] = carry
                carry = product[k : k + 1, :] * carry + state[k : k + 1, :]
            carries.append(entering)
        for k in range(SEGMENTS):
            span = pl.ds(k * pitch, steps)
            total = drive[0, c, span, :] + prefix[0, c, span, :] * carries[0][k]
            total = total + (drive[1, c, span, :] + prefix[1, c, span, :] * carries[1][k])
            mixed_ref[pl.ds(k * steps, steps), c * LANES : (c + 1) * LANES] = total.astype(jnp.bfloat16)
        if serve is not None:
            serve()


def recurrence_kernel(before_ref, taps_ref, rate_ref, recall_ref, admit_ref, mixed_ref, padded, decay, drive, prefix):
    length, width = before_ref.shape
    edge = jnp.zeros((PAD, width), jnp.float32)
    padded[pl.ds(0, PAD), :] = edge
    padded[pl.ds(PAD + length, PAD), :] = edge
    padded[pl.ds(PAD, length), :] = before_ref[...].astype(jnp.float32)
    gate_part(padded, taps_ref, rate_ref, recall_ref, admit_ref, decay, drive, length)
    scan_part(decay, drive, prefix, mixed_ref, length)


def recurrence(before, taps, rates, recall_maps, admit_maps):
    length, width = before.shape
    directions = rates.shape[0]
    chunks = width // LANES
    plane = pltpu.VMEM((directions, chunks, length, LANES), jnp.float32)
    return pl.pallas_call(
        recurrence_kernel,
        out_shape=jax.ShapeDtypeStruct((length, width), jnp.bfloat16),
        in_specs=[pl.BlockSpec(memory_space=pltpu.VMEM)] * 5,
        out_specs=pl.BlockSpec(memory_space=pltpu.VMEM),
        scratch_shapes=[pltpu.VMEM((length + 2 * PAD, width), jnp.float32), plane, plane, plane],
        compiler_params=pltpu.CompilerParams(vmem_limit_bytes=24 * 2**20),
        cost_estimate=pl.CostEstimate(flops=16 * length * width * 256, bytes_accessed=8 * 2**20, transcendentals=8 * length * width),
        name="recurrence",
    )(before, taps, rates, recall_maps, admit_maps)


def contract_last(left, right):
    return lax.dot_general(
        left, right, (((1,), (1,)), ((), ())), preferred_element_type=jnp.float32
    )


def gather(shard):
    copies = lax.axis_size("rep")
    if shard.shape[0] % (16 * copies):
        return lax.all_gather(shard.astype(jnp.bfloat16), "fs", axis=0, tiled=True)
    rows = shard.shape[0] // copies
    part = lax.dynamic_slice_in_dim(shard, lax.axis_index("rep") * rows, rows, 0)
    return lax.all_gather(part.astype(jnp.bfloat16), ("fs", "rep"), axis=0, tiled=True)


def body(
    tokens,
    first_gain,
    in_matrix,
    in_scale,
    conv_taps,
    decay_rate,
    recall_maps,
    admit_maps,
    out_matrix,
    out_scale,
    second_gain,
    up_matrix,
    up_scale,
    down_matrix,
    down_scale,
):
    stream = tokens.reshape(tokens.shape[1], tokens.shape[2]).astype(jnp.float32)
    factors = lax.all_gather(
        jnp.stack([out_scale, down_scale]).astype(jnp.bfloat16), "fs", axis=1, tiled=True
    )
    in_cols = gather(in_matrix)
    normed = normalize(stream, first_gain).astype(jnp.bfloat16)
    before = (
        jnp.dot(normed, in_cols, preferred_element_type=jnp.float32) * in_scale.astype(jnp.bfloat16)
    ).astype(jnp.bfloat16)
    mixed = recurrence(before, conv_taps, decay_rate, recall_maps, admit_maps)
    partial_value = contract_last(mixed, gather(out_matrix))
    middle = stream + factors[0] * lax.psum(partial_value.astype(jnp.bfloat16), "tp").astype(
        jnp.float32
    )
    second_normed = normalize(middle, second_gain).astype(jnp.bfloat16)
    raised = jnp.dot(second_normed, gather(up_matrix), preferred_element_type=jnp.float32)
    active = jnp.square(jax.nn.relu(raised * up_scale.astype(jnp.bfloat16))).astype(jnp.bfloat16)
    lowered = contract_last(active, gather(down_matrix))
    result = (
        middle + factors[1] * lax.psum(lowered.astype(jnp.bfloat16), "tp").astype(jnp.float32)
    ).astype(jnp.bfloat16)
    return result.reshape(tokens.shape)

MESH = pl.DeviceIdType.MESH
UNITS = 12
SPLIT = 2
OWN_TO_MATE = (2, 3, 4, 5, 6, 7, 8, 9)
OWN_TO_MATE_AFTER = {4: (10,), 7: (11,)}
OWN_TO_OTHER = (0, 1)
OWN_TO_OTHER_AFTER = {1: (2, 3), 3: (4, 5, 6), 6: (7,), 7: (8, 9, 10), 10: (11,)}
EDGE_SENDS = ((1, 2), (1, 3), (0, 2), (0, 3), (1, 4), (1, 5), (1, 6), (1, 7), (0, 4), (0, 5), (0, 6), (0, 7), (1, 8), (1, 9), (1, 10), (1, 11), (0, 8), (0, 9), (0, 10), (0, 11))
DOWN_ORDER = ((0, 0), (0, 1), None, (1, 0), (1, 1), (0, 2), (1, 2), (0, 3), (1, 3), (0, 4), (1, 4), (0, 5), (1, 5), (0, 6), (1, 6), (0, 7), (1, 7))
LAG = 8
EDGE_SERVES = (
    (2, 3, 4, 5, 6, 7, 8, 9, 14, 15),
    (),
    (),
    (26,),
    (),
    (27,),
    (),
    (),
    (),
    (16,),
    (),
    (),
    (),
    (17,),
    (),
    (),
    (),
    (),
    (),
    (18,),
    (),
    (),
    (),
    (28,),
    (),
    (),
    (),
    (10,),
    (),
    (29,),
    (),
    (30,),
    (19,),
    (),
    (),
    (),
    (31, 11, 20),
    (),
    (),
    (),
    (),
    (),
    (),
    (),
    (),
    (),
    (),
    (21,),
    (),
    (),
    (),
    (),
    (),
    (22,),
    (),
    (),
    (),
    (),
    (),
    (32,),
    (),
    (),
    (),
    (33, 34, 23),
    (),
    (),
    (),
    (),
    (),
    (),
    (),
    (35,),
    (),
    (),
    (),
    (),
    (),
    (),
    (),
    (),
    (),
    (),
    (),
    (),
    (),
    (),
    (),
    (),
    (),
    (),
    (),
    (),
    (),
)
INNER_SERVES = (
    (),
    (),
    (),
    (),
    (0, 12, 1, 13),
    (24, 25),
    (14,),
    (15,),
    (),
    (),
    (),
    (2,),
    (3,),
    (),
    (),
    (26,),
    (),
    (),
    (27,),
    (),
    (),
    (16, 4),
    (),
    (),
    (17, 5),
    (),
    (),
    (),
    (),
    (),
    (18,),
    (),
    (6,),
    (),
    (),
    (28,),
    (),
    (),
    (7,),
    (),
    (),
    (29,),
    (),
    (30,),
    (),
    (19,),
    (),
    (31,),
    (20, 8),
    (),
    (),
    (),
    (21,),
    (),
    (9,),
    (),
    (),
    (),
    (),
    (),
    (22, 10),
    (),
    (32, 11),
    (33,),
    (),
    (),
    (),
    (),
    (),
    (),
    (),
    (),
    (34,),
    (),
    (),
    (),
    (),
    (),
    (23,),
    (),
    (),
    (),
    (35,),
    (),
    (),
    (),
    (),
    (),
    (),
    (),
    (),
    (),
    (),
    (),
    (),
    (),
    (),
    (),
    (),
    (),
    (),
    (),
    (),
    (),
    (),
    (),
    (),
    (),
    (),
)


def layer_kernel(
    names, tokens_hbm, first_ref, in_hbm, in_scale_ref, taps_ref, rate_ref, recall_hbm, admit_hbm,
    out_hbm, out_scale_ref, second_ref, up_hbm, up_scale_ref, down_hbm, down_scale_ref,
    result_ref,
    tokens, in_own, out_own, up_own, down_own, recall_ref, admit_ref,
    in_all, out_all, up_all, down_all, scales_all, normed, guest, before, second_normed, padded, decay, drive, prefix,
    mixed, active, parts, near_parts, pairs, far_pairs, middle, load, send, recv,
):
    replica, place, rank = (lax.axis_index(name) for name in names)
    rep_name, fs_name, tp_name = names
    fs = 4
    length, model = tokens.shape
    block = model // fs
    half, quarter = block // 2, block // 4
    mate = place + 1 - 2 * lax.rem(place, 2)
    inner = lax.rem(lax.div(place + 1, 2), 2)
    other = fs - 1 - place
    other_mate = fs - 1 - mate
    slots = (mate, inner * other + (1 - inner) * other_mate, inner * other_mate + (1 - inner) * other)
    core = lax.rem(rank, 2)
    near = rank + 1 - 2 * core
    far = lax.rem(rank + 2, 4)
    sends, recvs = [0], [0]

    def fresh(counter):
        counter[0] += 1
        return counter[0] - 1

    def copy(src, dst, axis, peer, into=None):
        index = fresh(recvs) if into is None else into
        return pltpu.make_async_remote_copy(
            src_ref=src, dst_ref=dst, send_sem=send.at[fresh(sends)], recv_sem=recv.at[index],
            device_id={axis: peer}, device_id_type=MESH,
        )

    common_sent, edge_sent, inner_sent = [], [], []

    def start(one, sent=common_sent):
        one.start()
        sent.append(one)

    loads = [
        pltpu.make_async_copy(src, dst, load.at[i])
        for i, (src, dst) in enumerate((
            (in_hbm, in_own), (tokens_hbm, tokens), (out_hbm, out_own), (up_hbm, up_own), (down_hbm, down_own),
            (recall_hbm, recall_ref), (admit_hbm, admit_ref),
        ))
    ]
    for one in loads:
        one.start()
    load_in, load_tokens, load_out, load_up, load_down, load_recall, load_admit = loads

    barrier = pltpu.get_barrier_semaphore()
    greeted = [(rep_name, 1 - replica)]
    greeted += [(fs_name, lax.rem(place + k, fs)) for k in range(1, fs)]
    greeted += [(tp_name, near), (tp_name, far)]
    for axis, peer in greeted:
        pl.semaphore_signal(barrier, inc=1, device_id={axis: peer}, device_id_type=MESH)

    own_rows = pl.ds(pl.multiple_of(place * block, block), block)
    load_in.wait()
    in_all[own_rows, :] = in_own[...].astype(jnp.bfloat16)
    scales_all[place, 0:1, :] = out_scale_ref[...]
    scales_all[place, 1:2, :] = down_scale_ref[...]

    wide = up_all.shape[1] // 2

    def view(owner, unit, side):
        def rows(step):
            return pl.ds(pl.multiple_of(owner * block + side * half + step * quarter, quarter), quarter)

        if unit < 4:
            return (in_all, out_all)[unit // 2].at[rows(unit % 2), :]
        if unit < 8:
            return up_all.at[rows(unit % 2), (unit - 4) // 2 * wide : ((unit - 4) // 2 + 1) * wide]
        return down_all.at[rows((unit - 8) // 2), unit % 2 * wide : (unit % 2 + 1) * wide]

    to_mate, extra, to_other, pass_mate, pass_other, pass_last, swaps = [], [], [], [], [], [], []
    for unit in range(UNITS):
        into = [fresh(recvs) for _ in range(6)]
        own, first, second, third = (view(owner, unit, replica) for owner in (place,) + slots)
        rest = view(place, unit, 1 - replica)
        to_mate.append(copy(own, own, fs_name, mate, into[0]))
        extra.append(copy(rest, rest, fs_name, mate, into[3]))
        to_other.append(copy(own, own, fs_name, other, into[1]))
        pass_mate.append(copy(first, first, fs_name, other, into[2]))
        pass_other.append(copy(second, second, fs_name, mate, into[1]))
        pass_last.append(copy(third, third, fs_name, mate, into[2]))
        swaps.append([copy(part, part, rep_name, 1 - replica, into[3 + j]) for j, part in enumerate((first, second, third))])
    arrivals = (to_mate, to_other, pass_last)

    def serve_edge(codes):
        for code in codes:
            slot, unit = code // UNITS, code % UNITS
            arrivals[slot][unit].wait_recv()
            start(swaps[unit][slot], edge_sent)

    def serve_inner(codes):
        for code in codes:
            slot, unit = code // UNITS, code % UNITS
            arrivals[slot][unit].wait_recv()
            if slot or unit < SPLIT:
                start(swaps[unit][slot], inner_sent)
            if slot == 0:
                start(pass_mate[unit], inner_sent)
                for u in OWN_TO_OTHER_AFTER.get(unit, ()):
                    start(to_other[u], inner_sent)
            elif unit >= SPLIT:
                start((pass_other, pass_last)[slot - 1][unit], inner_sent)
            if slot == 2:
                for u in OWN_TO_MATE_AFTER.get(unit, ()):
                    start(to_mate[u], inner_sent)

    points = {"edge": 0, "inner": 0}

    def edge_next():
        points["edge"] += 1
        return EDGE_SERVES[points["edge"] - 1]

    def inner_next():
        points["inner"] += 1
        return INNER_SERVES[points["inner"] - 1]

    def serve():
        edge_codes, inner_codes = edge_next(), inner_next()
        if edge_codes:
            pl.when(inner == 0)(lambda: serve_edge(edge_codes))
        if inner_codes:
            pl.when(inner == 1)(lambda: serve_inner(inner_codes))

    def landed(units, taken=(0, 1, 2)):
        for unit in units:
            for slot in taken:
                swaps[unit][slot].wait_recv()

    piece = 32
    pieces = length // 4 // piece

    def guest_rows(owner, i):
        return pl.ds(pl.multiple_of(owner * (length // 4) + i * piece, piece), piece)

    tok, tok_far, tok_near, tok_onward = [], [], [], []
    for i in range(pieces):
        mine, theirs = guest_rows(rank, i), guest_rows(far, i)
        tok.append(copy(normed.at[mine, :], guest.at[mine, :], fs_name, mate))
        tok_far.append(copy(guest.at[mine, :], guest.at[mine, :], tp_name, far))
        tok_near.append(copy(guest.at[mine, :], guest.at[mine, :], tp_name, near))
        tok_onward.append(copy(guest.at[theirs, :], guest.at[theirs, :], tp_name, near))
    step = 256
    tiles = [slice(i * step, (i + 1) * step) for i in range(in_all.shape[1] // step)]
    given_before = [copy(before.at[:, at], before.at[:, at], fs_name, mate) for at in tiles]

    pl.semaphore_wait(barrier, len(greeted))

    @pl.when(inner == 0)
    def _():
        for unit in range(SPLIT):
            start(to_mate[unit], edge_sent)

    @pl.when(inner == 1)
    def _():
        for unit in OWN_TO_OTHER:
            start(to_other[unit], inner_sent)

    scale_copies = [
        copy(scales_all.at[place], scales_all.at[place], fs_name, lax.rem(place + k, fs)) for k in range(1, fs)
    ]
    for one in scale_copies:
        start(one)

    def norm_rows(at):
        normed[at, :] = normalize(tokens[at, :].astype(jnp.float32), first_ref[...]).astype(jnp.bfloat16)

    load_tokens.wait()

    @pl.when(inner == 0)
    def _():
        for i in range(pieces):
            norm_rows(guest_rows(rank, i))
            start(tok[i], edge_sent)

    load_out.wait()
    out_all[own_rows, :] = out_own[...].astype(jnp.bfloat16)

    @pl.when(inner == 1)
    def _():
        for unit in OWN_TO_MATE:
            if unit < 4:
                start(to_mate[unit], inner_sent)

    load_up.wait()
    up_all[own_rows, :] = up_own[...].astype(jnp.bfloat16)
    load_down.wait()
    down_all[own_rows, :] = down_own[...].astype(jnp.bfloat16)
    load_recall.wait()
    load_admit.wait()
    edge = jnp.zeros((PAD, padded.shape[1]), jnp.float32)
    padded[pl.ds(0, PAD), :] = edge
    padded[pl.ds(PAD + length, PAD), :] = edge

    @pl.when(inner == 0)
    def _():
        for whole, unit in EDGE_SENDS:
            start((to_mate if whole else extra)[unit], edge_sent)
        serve_edge(edge_next())
        for one, at in zip(given_before, tiles):
            one.wait_recv()
            padded[pl.ds(PAD, length), at] = before[:, at].astype(jnp.float32)

    @pl.when(inner == 1)
    def _():
        for unit in OWN_TO_MATE:
            if unit >= 4:
                start(to_mate[unit], inner_sent)
        tile = 64
        for i in range(4):

            def norm_step(k, _, i=i):
                norm_rows(pl.ds(pl.multiple_of((2 * i + k) * tile, tile), tile))
                return 0

            lax.fori_loop(0, length // tile // 4, norm_step, 0)
            serve_inner(inner_next())
        for i in range(pieces):
            serve_inner(inner_next())
            tok[i].wait_recv()
            start(tok_far[i], inner_sent)
            start(tok_near[i], inner_sent)
        for i in range(pieces):
            serve_inner(inner_next())
            tok_far[i].wait_recv()
            start(tok_onward[i], inner_sent)
        serve_inner(inner_next())
        landed(range(SPLIT))
        for one in tok_near + tok_onward:
            one.wait_recv()

        def project_in(values, at):
            product = jnp.dot(values[...], in_all[:, at], preferred_element_type=jnp.float32)
            return (product * in_scale_ref[:, at].astype(jnp.bfloat16).astype(jnp.float32)).astype(jnp.bfloat16)

        for one, at in zip(given_before, tiles):
            before[:, at] = project_in(guest, at)
            start(one, inner_sent)
            serve_inner(inner_next())
        for at in tiles:
            padded[pl.ds(PAD, length), at] = project_in(normed, at).astype(jnp.float32)
            serve_inner(inner_next())

    gate_part(padded, taps_ref, rate_ref, recall_ref, admit_ref, decay, drive, length, serve)
    scan_part(decay, drive, prefix, mixed, length, serve)

    serve()
    landed((2, 3))
    for one in scale_copies:
        one.wait_recv()
    chunks = model // step
    rows = length // 2
    batch = rows // 2
    kept = pl.ds(pl.multiple_of(core * rows, rows), rows)
    given = pl.ds(pl.multiple_of((1 - core) * rows, rows), rows)

    def of_batch(h):
        return slice(h * batch, (h + 1) * batch)

    def factor(owner, which, at):
        return scales_all[owner, which : which + 1, at].astype(jnp.bfloat16).astype(jnp.float32)

    to_near = [copy(parts.at[0, k, given, :], near_parts.at[0, k], tp_name, near) for k in range(chunks)]
    to_far = [
        [
            [copy(pairs.at[stage, k, of_batch(h), :], far_pairs.at[stage, k, of_batch(h), :], tp_name, far) for k in range(chunks)]
            for h in range(2)
        ]
        for stage in range(2)
    ]

    def far_total(stage, h, k):
        to_far[stage][h][k].wait_recv()
        return pairs[stage, k, of_batch(h), :].astype(jnp.float32) + far_pairs[stage, k, of_batch(h), :].astype(jnp.float32)

    for k in range(chunks + 2):
        if k < chunks:
            product = contract_last(mixed[...], out_all[k * step : (k + 1) * step, :])
            parts[0, k] = product.astype(jnp.bfloat16)
            start(to_near[k])
        serve()
        if k >= 2:
            to_near[k - 2].wait_recv()
            total = parts[0, k - 2, kept, :].astype(jnp.float32) + near_parts[0, k - 2].astype(jnp.float32)
            pairs[0, k - 2] = total.astype(jnp.bfloat16)
            start(to_far[0][0][k - 2])
    for k in range(chunks):
        start(to_far[0][1][k])

    spreads = []

    def middle_rows(h):
        squares = jnp.zeros((batch, 1), jnp.float32)
        at_rows = pl.ds(pl.multiple_of(core * rows + h * batch, batch), batch)
        for k in range(chunks):
            serve()
            at = slice(k * step, (k + 1) * step)
            inside = slice(k * step % block, k * step % block + step)
            value = tokens[at_rows, at].astype(jnp.float32) + factor(k * step // block, 0, inside) * far_total(0, h, k)
            middle[of_batch(h), at] = value
            squares = squares + jnp.sum(value * value, axis=1, keepdims=True)
        inverse = lax.rsqrt(squares * (1.0 / model) + EPSILON)
        at = pl.ds(pl.multiple_of(h * rows + core * batch, batch), batch)
        second_normed[at, :] = (middle[of_batch(h), :] * inverse * second_ref[...]).astype(jnp.bfloat16)
        spreads.append(copy(second_normed.at[at, :], second_normed.at[at, :], tp_name, near))
        start(spreads[h])

    def up_rows(h):
        serve()
        spreads[h].wait_recv()
        at_rows = slice(h * rows, (h + 1) * rows)
        for part in range(2):
            serve()
            if h == 0:
                landed((4 + 2 * part, 5 + 2 * part))
            for i in range(part * (wide // step), (part + 1) * (wide // step)):
                at = slice(i * step, (i + 1) * step)
                raised = jnp.dot(second_normed[at_rows, :], up_all[:, at], preferred_element_type=jnp.float32)
                raised = raised * up_scale_ref[:, at].astype(jnp.bfloat16).astype(jnp.float32)
                active[at_rows, at] = jnp.square(jnp.maximum(raised, 0.0)).astype(jnp.bfloat16)
                serve()

    middle_rows(0)
    up_rows(0)
    middle_rows(1)

    owners = [(place, 0, None), (place, 1, None)] + [(slots[j], q, j) for q in range(2) for j in range(3)]
    turns = [turn for turn in DOWN_ORDER if turn is not None]
    down_near, finals = [], []

    def pair_down(n):
        h, k = turns[n]
        serve()
        down_near[n].wait_recv()
        at = pl.ds(pl.multiple_of(h * rows + core * batch, batch), batch)
        total = parts[1, k, at, :].astype(jnp.float32) + near_parts[1, k, of_batch(h), :].astype(jnp.float32)
        pairs[1, k, of_batch(h), :] = total.astype(jnp.bfloat16)
        start(to_far[1][h][k])

    def finish(n):
        h, k = turns[n]
        owner, q, _ = owners[k]
        serve()
        total = far_total(1, h, k)
        at_rows = pl.ds(pl.multiple_of(core * rows + h * batch, batch), batch)
        for s in range(2):
            inside = slice(s * half + q * quarter, s * half + (q + 1) * quarter)
            at = pl.ds(pl.multiple_of(owner * block + s * half + q * quarter, quarter), quarter)
            value = middle[of_batch(h), at] + factor(owner, 1, inside) * total[:, s * quarter : (s + 1) * quarter]
            result_ref[at_rows, at] = value.astype(jnp.bfloat16)
            finals.append(copy(result_ref.at[at_rows, at], result_ref.at[at_rows, at], tp_name, near))
            start(finals[-1])

    n = 0
    for turn in DOWN_ORDER:
        if turn is None:
            up_rows(1)
            continue
        h, k = turn
        owner, q, j = owners[k]
        if j is not None and h == 0:
            serve()
            landed((8 + 2 * q, 9 + 2 * q), (j,))
        matrix = [
            down_all[pl.ds(pl.multiple_of(owner * block + s * half + q * quarter, quarter), quarter), :] for s in range(2)
        ]
        product = contract_last(active[h * rows : (h + 1) * rows, :], jnp.concatenate(matrix, axis=0))
        parts[1, k, h * rows : (h + 1) * rows, :] = product.astype(jnp.bfloat16)
        away = pl.ds(pl.multiple_of(h * rows + (1 - core) * batch, batch), batch)
        down_near.append(copy(parts.at[1, k, away, :], near_parts.at[1, k, of_batch(h), :], tp_name, near))
        start(down_near[n])
        if n >= 1:
            pair_down(n - 1)
        if n >= LAG:
            finish(n - LAG)
        n += 1
    pair_down(n - 1)
    for m in range(n - LAG, n):
        finish(m)
    serve()
    for one in finals:
        one.wait_recv()
    for one in common_sent:
        one.wait_send()

    @pl.when(inner == 0)
    def _():
        for one in edge_sent:
            one.wait_send()

    @pl.when(inner == 1)
    def _():
        for one in inner_sent:
            one.wait_send()


def fused_body(
    tokens, first_gain, in_matrix, in_scale, conv_taps, decay_rate, recall_maps, admit_maps,
    out_matrix, out_scale, second_gain, up_matrix, up_scale, down_matrix, down_scale,
):
    length, model = tokens.shape[1:]
    width, hidden = in_matrix.shape[1], up_matrix.shape[1]
    fs = lax.axis_size("fs")
    block, step = model // fs, 256
    directions = decay_rate.shape[0]
    plane = pltpu.VMEM((directions, width // LANES, SEGMENTS * (length // SEGMENTS + GAP), LANES), jnp.float32)
    gate = pltpu.VMEM(recall_maps.shape, jnp.float32)
    pieces = pltpu.VMEM((2, model // step, length // 2, step), jnp.bfloat16)
    rows = pltpu.VMEM((length, model), jnp.bfloat16)
    channels = pltpu.VMEM((length, width), jnp.bfloat16)
    vmem, hbm = pl.BlockSpec(memory_space=pltpu.VMEM), pl.BlockSpec(memory_space=pl.ANY)
    count = UNITS * 7 + 3 + 16 + 2 + 9 * (model // step) + 2 + 4 * (model // step)
    result = pl.pallas_call(
        functools.partial(layer_kernel, ("rep", "fs", "tp")),
        out_shape=pltpu.VMEM((length, model), jnp.bfloat16),
        in_specs=[hbm, vmem, hbm, vmem, vmem, vmem, hbm, hbm, hbm, vmem, vmem, hbm, vmem, hbm, vmem],
        out_specs=vmem,
        scratch_shapes=[
            rows,
            pltpu.VMEM((block, width), jnp.float32),
            pltpu.VMEM((block, width), jnp.float32),
            pltpu.VMEM((block, hidden), jnp.float32),
            pltpu.VMEM((block, hidden), jnp.float32),
            gate, gate,
            pltpu.VMEM((model, width), jnp.bfloat16),
            pltpu.VMEM((model, width), jnp.bfloat16),
            pltpu.VMEM((model, hidden), jnp.bfloat16),
            pltpu.VMEM((model, hidden), jnp.bfloat16),
            pltpu.VMEM((fs, 2, block), jnp.float32),
            rows, rows, channels, rows,
            pltpu.VMEM((length + 2 * PAD, width), jnp.float32),
            plane, plane, plane,
            channels,
            pltpu.VMEM((length, hidden), jnp.bfloat16),
            pltpu.VMEM((2, model // step, length, step), jnp.bfloat16),
            pieces, pieces, pieces,
            pltpu.VMEM((length // 2, model), jnp.float32),
            pltpu.SemaphoreType.DMA((7,)),
            pltpu.SemaphoreType.DMA((count + 3 * UNITS,)),
            pltpu.SemaphoreType.DMA((count,)),
        ],
        compiler_params=pltpu.CompilerParams(
            collective_id=0, has_side_effects=True, vmem_limit_bytes=59 * 2**20
        ),
        name="layer",
    )(
        tokens.reshape(length, model), first_gain[None], in_matrix, in_scale[None], conv_taps, decay_rate,
        recall_maps, admit_maps, out_matrix, out_scale[None], second_gain[None], up_matrix, up_scale[None], down_matrix,
        down_scale[None],
    )
    return result.reshape(tokens.shape)


def solution(mesh):
    placed = (
        P(("rep", "fs"), None, None),
        P(),
        P("fs", "tp"),
        P("tp"),
        P(None, "tp"),
        P(None, "tp"),
        P(None, "tp", None, None),
        P(None, "tp", None, None),
        P("fs", "tp"),
        P("fs"),
        P(),
        P("fs", "tp"),
        P("tp"),
        P("fs", "tp"),
        P("fs"),
    )
    small = (mesh.shape["rep"], mesh.shape["fs"], mesh.shape["tp"]) == (2, 4, 4)
    return jax.shard_map(
        fused_body if small else body, mesh=mesh, in_specs=placed, out_specs=P(("rep", "fs"), None, None), check_vma=False
    )
```

```python
import functools
import math
import jax
import jax.numpy as jnp
from jax import lax
from jax.experimental import pallas as pl
from jax.experimental.pallas import tpu as pltpu
from jax.sharding import PartitionSpec as P

EPSILON = 1e-06
RATE_GAIN = 8.0
LANES = 128
SEGMENTS = 8
PAD = 8
GAP = 8


def normalize(stream, gain):
    return stream * lax.rsqrt(jnp.mean(stream * stream, axis=-1, keepdims=True) + EPSILON) * gain


def one_minus_exp(y):
    series = 1.0 + y * (1.0 / 6.0)
    for k in (5.0, 4.0, 3.0, 2.0):
        series = 1.0 + y * (1.0 / k) * series
    return jnp.where(y > -0.25, -y * series, 1.0 - jnp.exp(y))


def sigmoid(x):
    return 0.5 * jnp.tanh(0.5 * x) + 0.5


def gate_part(padded, taps_ref, rate_ref, recall_ref, admit_ref, decay, drive, length, serve=None):
    directions, groups, block, _ = recall_ref.shape
    taps = taps_ref.shape[0]
    rows = length // SEGMENTS
    pitch = decay.shape[2] // SEGMENTS

    def tile_step(tile, _):
        base = pl.multiple_of(tile * rows, rows)
        into = pl.multiple_of(tile * pitch, 8)
        conv = jnp.zeros((rows, padded.shape[1]), jnp.float32)
        window = padded[pl.ds(base, rows + 2 * PAD), :]
        for k in range(taps):
            first = PAD - taps // 2 + k
            conv = conv + taps_ref[k : k + 1, :] * window[first : first + rows, :]
        narrow = conv.astype(jnp.bfloat16)
        for g in range(groups):
            values = conv[:, g * block : (g + 1) * block]
            left = narrow[:, g * block : (g + 1) * block]
            for d in range(directions):
                recall = sigmoid(jnp.dot(left, recall_ref[d, g].astype(jnp.bfloat16), preferred_element_type=jnp.float32))
                admit = sigmoid(jnp.dot(left, admit_ref[d, g].astype(jnp.bfloat16), preferred_element_type=jnp.float32))
                log_decay = recall * (-RATE_GAIN * rate_ref[d : d + 1, g * block : (g + 1) * block])
                a = jnp.exp(log_decay)
                b = jnp.sqrt(one_minus_exp(2.0 * log_decay)) * admit * values
                for c in range(block // LANES):
                    where = g * (block // LANES) + c
                    decay[d, where, pl.ds(into, rows), :] = a[:, c * LANES : (c + 1) * LANES]
                    drive[d, where, pl.ds(into, rows), :] = b[:, c * LANES : (c + 1) * LANES]
        return 0

    if serve is None:
        lax.fori_loop(0, SEGMENTS, tile_step, 0)
        return
    for first in range(0, SEGMENTS, 2):
        lax.fori_loop(first, first + 2, tile_step, 0)
        serve()


def scan_part(decay, drive, prefix, mixed_ref, length, serve=None):
    directions, chunks = decay.shape[:2]
    steps = length // SEGMENTS
    pitch = decay.shape[2] // SEGMENTS
    lanes = [(d, c) for d in range(directions) for c in range(chunks)]

    def scan_step(s, carried):
        out = []
        for (d, c), (state, product) in zip(lanes, carried):
            at = s if d == 0 else steps - 1 - s
            a = decay[d, c, pl.ds(at, SEGMENTS, stride=pitch), :]
            b = drive[d, c, pl.ds(at, SEGMENTS, stride=pitch), :]
            state = a * state + b
            product = a * product
            drive[d, c, pl.ds(at, SEGMENTS, stride=pitch), :] = state
            prefix[d, c, pl.ds(at, SEGMENTS, stride=pitch), :] = product
            out.append((state, product))
        return tuple(out)

    start = tuple((jnp.zeros((SEGMENTS, LANES), jnp.float32), jnp.ones((SEGMENTS, LANES), jnp.float32)) for _ in lanes)
    if serve is None:
        ends = lax.fori_loop(0, steps, scan_step, start, unroll=4)
    else:
        ends = start
        for first in range(0, steps, steps // 4):
            ends = lax.fori_loop(first, first + steps // 4, scan_step, ends, unroll=4)
            serve()
    ends = dict(zip(lanes, ends))

    for c in range(chunks):
        carries = []
        for d in range(directions):
            state, product = ends[(d, c)]
            order = range(SEGMENTS) if d == 0 else range(SEGMENTS - 1, -1, -1)
            carry = jnp.zeros((1, LANES), jnp.float32)
            entering = {}
            for k in order:
                entering[k] = carry
                carry = product[k : k + 1, :] * carry + state[k : k + 1, :]
            carries.append(entering)
        for k in range(SEGMENTS):
            span = pl.ds(k * pitch, steps)
            total = drive[0, c, span, :] + prefix[0, c, span, :] * carries[0][k]
            total = total + (drive[1, c, span, :] + prefix[1, c, span, :] * carries[1][k])
            mixed_ref[pl.ds(k * steps, steps), c * LANES : (c + 1) * LANES] = total.astype(jnp.bfloat16)
        if serve is not None:
            serve()


def recurrence_kernel(before_ref, taps_ref, rate_ref, recall_ref, admit_ref, mixed_ref, padded, decay, drive, prefix):
    length, width = before_ref.shape
    edge = jnp.zeros((PAD, width), jnp.float32)
    padded[pl.ds(0, PAD), :] = edge
    padded[pl.ds(PAD + length, PAD), :] = edge
    padded[pl.ds(PAD, length), :] = before_ref[...].astype(jnp.float32)
    gate_part(padded, taps_ref, rate_ref, recall_ref, admit_ref, decay, drive, length)
    scan_part(decay, drive, prefix, mixed_ref, length)


def recurrence(before, taps, rates, recall_maps, admit_maps):
    length, width = before.shape
    directions = rates.shape[0]
    chunks = width // LANES
    plane = pltpu.VMEM((directions, chunks, length, LANES), jnp.float32)
    return pl.pallas_call(
        recurrence_kernel,
        out_shape=jax.ShapeDtypeStruct((length, width), jnp.bfloat16),
        in_specs=[pl.BlockSpec(memory_space=pltpu.VMEM)] * 5,
        out_specs=pl.BlockSpec(memory_space=pltpu.VMEM),
        scratch_shapes=[pltpu.VMEM((length + 2 * PAD, width), jnp.float32), plane, plane, plane],
        compiler_params=pltpu.CompilerParams(vmem_limit_bytes=24 * 2**20),
        cost_estimate=pl.CostEstimate(flops=16 * length * width * 256, bytes_accessed=8 * 2**20, transcendentals=8 * length * width),
        name="recurrence",
    )(before, taps, rates, recall_maps, admit_maps)


def contract_last(left, right):
    return lax.dot_general(
        left, right, (((1,), (1,)), ((), ())), preferred_element_type=jnp.float32
    )


def gather(shard):
    copies = lax.axis_size("rep")
    if shard.shape[0] % (16 * copies):
        return lax.all_gather(shard.astype(jnp.bfloat16), "fs", axis=0, tiled=True)
    rows = shard.shape[0] // copies
    part = lax.dynamic_slice_in_dim(shard, lax.axis_index("rep") * rows, rows, 0)
    return lax.all_gather(part.astype(jnp.bfloat16), ("fs", "rep"), axis=0, tiled=True)


def body(
    tokens,
    first_gain,
    in_matrix,
    in_scale,
    conv_taps,
    decay_rate,
    recall_maps,
    admit_maps,
    out_matrix,
    out_scale,
    second_gain,
    up_matrix,
    up_scale,
    down_matrix,
    down_scale,
):
    stream = tokens.reshape(tokens.shape[1], tokens.shape[2]).astype(jnp.float32)
    factors = lax.all_gather(
        jnp.stack([out_scale, down_scale]).astype(jnp.bfloat16), "fs", axis=1, tiled=True
    )
    in_cols = gather(in_matrix)
    normed = normalize(stream, first_gain).astype(jnp.bfloat16)
    before = (
        jnp.dot(normed, in_cols, preferred_element_type=jnp.float32) * in_scale.astype(jnp.bfloat16)
    ).astype(jnp.bfloat16)
    mixed = recurrence(before, conv_taps, decay_rate, recall_maps, admit_maps)
    partial_value = contract_last(mixed, gather(out_matrix))
    middle = stream + factors[0] * lax.psum(partial_value.astype(jnp.bfloat16), "tp").astype(
        jnp.float32
    )
    second_normed = normalize(middle, second_gain).astype(jnp.bfloat16)
    raised = jnp.dot(second_normed, gather(up_matrix), preferred_element_type=jnp.float32)
    active = jnp.square(jax.nn.relu(raised * up_scale.astype(jnp.bfloat16))).astype(jnp.bfloat16)
    lowered = contract_last(active, gather(down_matrix))
    result = (
        middle + factors[1] * lax.psum(lowered.astype(jnp.bfloat16), "tp").astype(jnp.float32)
    ).astype(jnp.bfloat16)
    return result.reshape(tokens.shape)

MESH = pl.DeviceIdType.MESH
UNITS = 14
SPLIT = 2
OWN_TO_MATE = (2, 3, 4, 5, 6, 7, 8, 9, 10)
OWN_TO_MATE_AFTER = {6: (11,), 8: (12,), 5: (13,)}
OWN_TO_OTHER = (0, 1)
OWN_TO_OTHER_AFTER = {1: (2, 3), 3: (4, 5), 4: (6,), 6: (7,), 7: (8, 9), 8: (10,), 10: (11,), 11: (12, 13)}
EDGE_SENDS = ((1, 2), (1, 3), (0, 2), (0, 3), (1, 4), (1, 5), (1, 6), (1, 7), (0, 4), (0, 5), (0, 6), (0, 7), (1, 8), (1, 9), (1, 10), (1, 11), (1, 12), (1, 13), (0, 8), (0, 9), (0, 10), (0, 11), (0, 12), (0, 13))
DOWN_ORDER = ((0, 0), (0, 1), None, (1, 0), (1, 1), (0, 2), (1, 2), (0, 3), (1, 3), (0, 4), (1, 4), (0, 5), (1, 5), (0, 6), (1, 6), (0, 7), (1, 7))
LAG = 8
EDGE_SERVES = (
    (2, 3, 4, 5, 6, 7, 8, 9, 10, 16, 17),
    (),
    (),
    (30,),
    (),
    (31,),
    (),
    (),
    (),
    (18,),
    (),
    (),
    (),
    (19,),
    (),
    (),
    (),
    (),
    (),
    (32,),
    (),
    (),
    (),
    (20,),
    (),
    (),
    (),
    (33,),
    (13,),
    (),
    (34,),
    (11,),
    (21,),
    (),
    (),
    (),
    (35, 22, 23),
    (),
    (),
    (),
    (),
    (),
    (),
    (),
    (),
    (),
    (),
    (36, 12),
    (),
    (),
    (),
    (),
    (),
    (24,),
    (),
    (),
    (),
    (),
    (),
    (37,),
    (),
    (),
    (38,),
    (25, 39, 26),
    (),
    (),
    (27,),
    (),
    (),
    (),
    (),
    (40,),
    (),
    (41,),
    (),
    (),
    (),
    (),
    (),
    (),
    (),
    (),
    (),
    (),
    (),
    (),
    (),
    (),
    (),
    (),
    (),
    (),
    (),
)
INNER_SERVES = (
    (),
    (),
    (),
    (),
    (0, 14, 1, 15),
    (28, 29),
    (16,),
    (17,),
    (),
    (),
    (),
    (2,),
    (3,),
    (),
    (),
    (30,),
    (),
    (),
    (31,),
    (),
    (),
    (18, 4),
    (),
    (),
    (19, 5),
    (),
    (),
    (),
    (),
    (),
    (32,),
    (),
    (6,),
    (),
    (),
    (20,),
    (),
    (),
    (7,),
    (),
    (),
    (33,),
    (),
    (34,),
    (),
    (21,),
    (),
    (35,),
    (22, 8),
    (),
    (),
    (),
    (),
    (23,),
    (9,),
    (),
    (),
    (),
    (),
    (10,),
    (36, 11),
    (24, 12),
    (13,),
    (37, 38),
    (),
    (),
    (25,),
    (),
    (),
    (),
    (),
    (),
    (39,),
    (),
    (),
    (26,),
    (),
    (),
    (27, 40),
    (),
    (),
    (),
    (41,),
    (),
    (),
    (),
    (),
    (),
    (),
    (),
    (),
    (),
    (),
    (),
    (),
    (),
    (),
    (),
    (),
    (),
    (),
    (),
    (),
    (),
    (),
    (),
    (),
    (),
    (),
)


def layer_kernel(
    names, tokens_hbm, first_hbm, in_hbm, in_scale_hbm, taps_hbm, rate_hbm, recall_hbm, admit_hbm,
    out_hbm, out_scale_hbm, second_hbm, up_hbm, up_scale_hbm, down_hbm, down_scale_hbm,
    result_ref,
    first_ref, in_scale_ref, taps_ref, rate_ref, second_ref, up_scale_ref, tokens, in_own, out_own, up_own, down_own, recall_ref, admit_ref,
    in_all, out_all, up_all, down_all, scales_all, normed, guest, before, second_normed, padded, decay, drive, prefix,
    mixed, active, parts, near_parts, pairs, far_pairs, middle, load, send, recv,
):
    replica, place, rank = (lax.axis_index(name) for name in names)
    rep_name, fs_name, tp_name = names
    fs = 4
    length, model = tokens.shape
    block = model // fs
    half, quarter = block // 2, block // 4
    mate = place + 1 - 2 * lax.rem(place, 2)
    inner = lax.rem(lax.div(place + 1, 2), 2)
    other = fs - 1 - place
    other_mate = fs - 1 - mate
    slots = (mate, inner * other + (1 - inner) * other_mate, inner * other_mate + (1 - inner) * other)
    core = lax.rem(rank, 2)
    near = rank + 1 - 2 * core
    far = lax.rem(rank + 2, 4)
    recvs, groups = [0], {}

    def fresh():
        recvs[0] += 1
        return recvs[0] - 1

    def whole_copy(src, dst, axis, peer, group, into):
        return pltpu.make_async_remote_copy(
            src_ref=src, dst_ref=dst, send_sem=send.at[groups.setdefault(group, len(groups))], recv_sem=recv.at[into],
            device_id={axis: peer}, device_id_type=MESH,
        )

    def bytes_of(ref):
        return math.prod(ref.shape) * jnp.dtype(ref.dtype).itemsize

    def waiter(size, group, into):
        count = size // bytes_of(up_all.at[0])
        return whole_copy(up_all.at[0:count, :], up_all.at[0:count, :], tp_name, near, group, into)

    class copy:
        def __init__(self, src, dst, axis, peer, group, into=None):
            self.into = fresh() if into is None else into
            self.group, self.size = group, bytes_of(src)
            self.one = whole_copy(src, dst, axis, peer, group, self.into)
            self.start, self.wait_recv, self.wait_send = self.one.start, self.one.wait_recv, self.one.wait_send

    common_sent, edge_sent, inner_sent = {}, {}, {}

    def start(one, sent=common_sent):
        one.start()
        sent.setdefault(one.group, []).append(one)

    def drain(sent):
        for group, copies in sent.items():
            if len(copies) == 1:
                copies[0].wait_send()
            else:
                waiter(sum(one.size for one in copies), group, copies[0].into).wait_send()

    def wait_all(copies):
        waiter(sum(one.size for one in copies), copies[0].group, copies[0].into).wait_recv()

    barrier = pltpu.get_barrier_semaphore()
    greeted = [(rep_name, 1 - replica)]
    greeted += [(fs_name, mate), (tp_name, near), (tp_name, far)]

    def greet(axis, peer):
        pl.semaphore_signal(barrier, inc=1, device_id={axis: peer}, device_id_type=MESH)

    for axis, peer in greeted:
        greet(axis, peer)
    pl.when(inner == 1)(lambda: greet(fs_name, other))

    loads = [
        pltpu.make_async_copy(src, dst, load.at[i])
        for i, (src, dst) in enumerate((
            (in_hbm, in_own), (out_hbm, out_own), (first_hbm, first_ref), (tokens_hbm, tokens), (up_hbm, up_own),
            (down_hbm, down_own), (out_scale_hbm, scales_all.at[place, 0:1, :]), (down_scale_hbm, scales_all.at[place, 1:2, :]),
            (in_scale_hbm, in_scale_ref), (taps_hbm, taps_ref), (rate_hbm, rate_ref), (second_hbm, second_ref),
            (up_scale_hbm, up_scale_ref), (recall_hbm, recall_ref), (admit_hbm, admit_ref),
        ))
    ]
    for one in loads:
        one.start()
    load_in, load_out, load_first, load_tokens, load_up, load_down = loads[:6]
    load_scales, load_rest = loads[6:8], loads[8:]

    own_rows = pl.ds(pl.multiple_of(place * block, block), block)
    load_in.wait()
    in_all[own_rows, :] = in_own[...].astype(jnp.bfloat16)
    load_out.wait()
    out_all[own_rows, :] = out_own[...].astype(jnp.bfloat16)

    wide = up_all.shape[1] // 2

    def view(owner, unit, side):
        def rows(first, count):
            return pl.ds(pl.multiple_of(owner * block + side * half + first, count), count)

        def columns(part):
            return slice(part * wide, (part + 1) * wide)

        if unit < 4:
            return (in_all, out_all)[unit // 2].at[rows(unit % 2 * quarter, quarter), :]
        if unit < 8:
            return up_all.at[rows(unit % 2 * quarter, quarter), columns((unit - 4) // 2)]
        if unit < 10:
            return down_all.at[rows(0, quarter), columns(unit - 8)]
        return down_all.at[rows(quarter + (unit - 10) % 2 * (quarter // 2), quarter // 2), columns((unit - 10) // 2)]

    to_mate, extra, to_other, pass_mate, pass_other, pass_last, swaps = [], [], [], [], [], [], []
    bundles = [(0, 1), (2, 3), (4, 5), (6, 7), (8, 9), tuple(range(10, UNITS))]
    landings = {}
    for bundle in bundles:
        shared = [fresh() for _ in range(3 if bundle[0] >= 8 else 1)] * (1 if bundle[0] >= 8 else 3)
        for unit in bundle:
            landings[unit] = shared
    for unit in range(UNITS):
        into = [fresh() for _ in range(3)]
        own, first, second, third = (view(owner, unit, replica) for owner in (place,) + slots)
        rest = view(place, unit, 1 - replica)
        land = landings[unit]
        to_mate.append(copy(own, own, fs_name, mate, "to_mate", into[0]))
        extra.append(copy(rest, rest, fs_name, mate, "extra", land[0]) if unit >= SPLIT else None)
        to_other.append(copy(own, own, fs_name, other, "to_other", into[1]))
        pass_mate.append(copy(first, first, fs_name, other, "pass_mate", into[2]))
        pass_other.append(copy(second, second, fs_name, mate, "pass_other", into[1]) if unit >= SPLIT else None)
        pass_last.append(copy(third, third, fs_name, mate, "pass_last", into[2]))
        swaps.append([copy(part, part, rep_name, 1 - replica, f"swap{j}", land[j]) for j, part in enumerate((first, second, third))])
    arrivals = (to_mate, to_other, pass_last)

    def serve_edge(codes):
        for code in codes:
            slot, unit = code // UNITS, code % UNITS
            arrivals[slot][unit].wait_recv()
            start(swaps[unit][slot], edge_sent)

    def serve_inner(codes):
        for code in codes:
            slot, unit = code // UNITS, code % UNITS
            arrivals[slot][unit].wait_recv()
            if slot or unit < SPLIT:
                start(swaps[unit][slot], inner_sent)
            if slot == 0:
                start(pass_mate[unit], inner_sent)
                for u in OWN_TO_OTHER_AFTER.get(unit, ()):
                    start(to_other[u], inner_sent)
            elif unit >= SPLIT:
                start((pass_other, pass_last)[slot - 1][unit], inner_sent)
            if slot == 2:
                for u in OWN_TO_MATE_AFTER.get(unit, ()):
                    start(to_mate[u], inner_sent)

    points = {"edge": 0, "inner": 0}

    def edge_next():
        points["edge"] += 1
        return EDGE_SERVES[points["edge"] - 1]

    def inner_next():
        points["inner"] += 1
        return INNER_SERVES[points["inner"] - 1]

    def serve():
        edge_codes, inner_codes = edge_next(), inner_next()
        if edge_codes:
            pl.when(inner == 0)(lambda: serve_edge(edge_codes))
        if inner_codes:
            pl.when(inner == 1)(lambda: serve_inner(inner_codes))

    def landed(units, taken=(0, 1, 2)):
        wait_all([swaps[unit][slot] for unit in units for slot in taken])

    piece = 32
    pieces = length // 4 // piece

    def guest_rows(owner, i):
        return pl.ds(pl.multiple_of(owner * (length // 4) + i * piece, piece), piece)

    tok, tok_far, tok_near, tok_onward = [], [], [], []
    guest_near = fresh()
    for i in range(pieces):
        mine, theirs = guest_rows(rank, i), guest_rows(far, i)
        tok.append(copy(normed.at[mine, :], guest.at[mine, :], fs_name, mate, "guest"))
        tok_far.append(copy(guest.at[mine, :], guest.at[mine, :], tp_name, far, "guest"))
        tok_near.append(copy(guest.at[mine, :], guest.at[mine, :], tp_name, near, "guest", guest_near))
        tok_onward.append(copy(guest.at[theirs, :], guest.at[theirs, :], tp_name, near, "guest", guest_near))
    step = 256
    tiles = [slice(i * step, (i + 1) * step) for i in range(in_all.shape[1] // step)]
    given_before = [copy(before.at[:, at], before.at[:, at], fs_name, mate, "guest") for at in tiles]

    pl.when(inner == 0)(lambda: pl.semaphore_wait(barrier, len(greeted)))
    pl.when(inner == 1)(lambda: pl.semaphore_wait(barrier, len(greeted) + 1))

    @pl.when(inner == 0)
    def _():
        for unit in range(SPLIT):
            start(to_mate[unit], edge_sent)

    @pl.when(inner == 1)
    def _():
        for unit in OWN_TO_OTHER:
            start(to_other[unit], inner_sent)
        for unit in OWN_TO_MATE:
            if unit < 4:
                start(to_mate[unit], inner_sent)

    def norm_rows(at):
        normed[at, :] = normalize(tokens[at, :].astype(jnp.float32), first_ref[...]).astype(jnp.bfloat16)

    load_first.wait()
    load_tokens.wait()

    @pl.when(inner == 0)
    def _():
        for i in range(pieces):
            norm_rows(guest_rows(rank, i))
            start(tok[i], edge_sent)

    load_up.wait()
    up_all[own_rows, :] = up_own[...].astype(jnp.bfloat16)
    load_down.wait()
    down_all[own_rows, :] = down_own[...].astype(jnp.bfloat16)
    for one in load_scales:
        one.wait()
    into = [fresh() for _ in range(3)]
    own, first, second, third = (scales_all.at[owner] for owner in (place,) + slots)
    scale_in = [
        copy(own, own, fs_name, mate, "scale0", into[0]), copy(own, own, fs_name, other, "scale1", into[1]),
        copy(third, third, fs_name, mate, "scale2", into[2]),
    ]
    scale_out = [
        copy(first, first, fs_name, other, "scale3", into[2]), copy(second, second, fs_name, mate, "scale4", into[1]), scale_in[2],
    ]
    start(scale_in[0])
    pl.when(inner == 1)(lambda: start(scale_in[1], inner_sent))

    def pass_scales(slot):
        scale_in[slot].wait_recv()
        start(scale_out[slot], inner_sent)

    for one in load_rest:
        one.wait()
    edge = jnp.zeros((PAD, padded.shape[1]), jnp.float32)
    padded[pl.ds(0, PAD), :] = edge
    padded[pl.ds(PAD + length, PAD), :] = edge

    @pl.when(inner == 0)
    def _():
        for whole, unit in EDGE_SENDS:
            start((to_mate if whole else extra)[unit], edge_sent)
        serve_edge(edge_next())
        for one, at in zip(given_before, tiles):
            one.wait_recv()
            padded[pl.ds(PAD, length), at] = before[:, at].astype(jnp.float32)

    @pl.when(inner == 1)
    def _():
        for unit in OWN_TO_MATE:
            if unit >= 4:
                start(to_mate[unit], inner_sent)
        tile = 64
        for i in range(4):

            def norm_step(k, _, i=i):
                norm_rows(pl.ds(pl.multiple_of((2 * i + k) * tile, tile), tile))
                return 0

            lax.fori_loop(0, length // tile // 4, norm_step, 0)
            serve_inner(inner_next())
        for i in range(pieces):
            serve_inner(inner_next())
            tok[i].wait_recv()
            start(tok_far[i], inner_sent)
            start(tok_near[i], inner_sent)
        pass_scales(0)
        pass_scales(1)
        for i in range(pieces):
            serve_inner(inner_next())
            tok_far[i].wait_recv()
            start(tok_onward[i], inner_sent)
        serve_inner(inner_next())
        landed(range(SPLIT))
        wait_all(tok_near + tok_onward)

        def project_in(values, at):
            product = jnp.dot(values[...], in_all[:, at], preferred_element_type=jnp.float32)
            return (product * in_scale_ref[:, at].astype(jnp.bfloat16).astype(jnp.float32)).astype(jnp.bfloat16)

        for one, at in zip(given_before, tiles):
            before[:, at] = project_in(guest, at)
            start(one, inner_sent)
            serve_inner(inner_next())
        pass_scales(2)
        for at in tiles:
            padded[pl.ds(PAD, length), at] = project_in(normed, at).astype(jnp.float32)
            serve_inner(inner_next())

    gate_part(padded, taps_ref, rate_ref, recall_ref, admit_ref, decay, drive, length, serve)
    scan_part(decay, drive, prefix, mixed, length, serve)

    serve()
    landed((2, 3))

    @pl.when(inner == 0)
    def _():
        for one in scale_in:
            one.wait_recv()

    chunks = model // step
    rows = length // 2
    batch = rows // 2
    kept = pl.ds(pl.multiple_of(core * rows, rows), rows)
    given = pl.ds(pl.multiple_of((1 - core) * rows, rows), rows)

    def of_batch(h):
        return slice(h * batch, (h + 1) * batch)

    def factor(owner, which, at):
        return scales_all[owner, which : which + 1, at].astype(jnp.bfloat16).astype(jnp.float32)

    to_near = [copy(parts.at[0, k, given, :], near_parts.at[0, k], tp_name, near, "reduce") for k in range(chunks)]
    to_far = [
        [
            [copy(pairs.at[stage, k, of_batch(h), :], far_pairs.at[stage, k, of_batch(h), :], tp_name, far, "reduce") for k in range(chunks)]
            for h in range(2)
        ]
        for stage in range(2)
    ]

    def far_total(stage, h, k):
        to_far[stage][h][k].wait_recv()
        return pairs[stage, k, of_batch(h), :].astype(jnp.float32) + far_pairs[stage, k, of_batch(h), :].astype(jnp.float32)

    for k in range(chunks + 2):
        if k < chunks:
            product = contract_last(mixed[...], out_all[k * step : (k + 1) * step, :])
            parts[0, k] = product.astype(jnp.bfloat16)
            start(to_near[k])
        serve()
        if k >= 2:
            to_near[k - 2].wait_recv()
            total = parts[0, k - 2, kept, :].astype(jnp.float32) + near_parts[0, k - 2].astype(jnp.float32)
            pairs[0, k - 2] = total.astype(jnp.bfloat16)
            start(to_far[0][0][k - 2])
    for k in range(chunks):
        start(to_far[0][1][k])

    spreads = []

    def middle_rows(h):
        squares = jnp.zeros((batch, 1), jnp.float32)
        at_rows = pl.ds(pl.multiple_of(core * rows + h * batch, batch), batch)
        for k in range(chunks):
            serve()
            at = slice(k * step, (k + 1) * step)
            inside = slice(k * step % block, k * step % block + step)
            value = tokens[at_rows, at].astype(jnp.float32) + factor(k * step // block, 0, inside) * far_total(0, h, k)
            middle[of_batch(h), at] = value
            squares = squares + jnp.sum(value * value, axis=1, keepdims=True)
        inverse = lax.rsqrt(squares * (1.0 / model) + EPSILON)
        at = pl.ds(pl.multiple_of(h * rows + core * batch, batch), batch)
        second_normed[at, :] = (middle[of_batch(h), :] * inverse * second_ref[...]).astype(jnp.bfloat16)
        spreads.append(copy(second_normed.at[at, :], second_normed.at[at, :], tp_name, near, "spread"))
        start(spreads[h])

    def up_rows(h):
        serve()
        spreads[h].wait_recv()
        at_rows = slice(h * rows, (h + 1) * rows)
        for part in range(2):
            serve()
            if h == 0:
                landed((4 + 2 * part, 5 + 2 * part))
            for i in range(part * (wide // step), (part + 1) * (wide // step)):
                at = slice(i * step, (i + 1) * step)
                raised = jnp.dot(second_normed[at_rows, :], up_all[:, at], preferred_element_type=jnp.float32)
                raised = raised * up_scale_ref[:, at].astype(jnp.bfloat16).astype(jnp.float32)
                active[at_rows, at] = jnp.square(jnp.maximum(raised, 0.0)).astype(jnp.bfloat16)
                serve()

    middle_rows(0)
    up_rows(0)
    middle_rows(1)

    owners = [(place, 0, None), (place, 1, None)] + [(slots[j], q, j) for q in range(2) for j in range(3)]
    turns = [turn for turn in DOWN_ORDER if turn is not None]
    down_near, finals, final = [], [], fresh()

    def pair_down(n):
        h, k = turns[n]
        serve()
        down_near[n].wait_recv()
        at = pl.ds(pl.multiple_of(h * rows + core * batch, batch), batch)
        total = parts[1, k, at, :].astype(jnp.float32) + near_parts[1, k, of_batch(h), :].astype(jnp.float32)
        pairs[1, k, of_batch(h), :] = total.astype(jnp.bfloat16)
        start(to_far[1][h][k])

    def finish(n):
        h, k = turns[n]
        owner, q, _ = owners[k]
        serve()
        total = far_total(1, h, k)
        at_rows = pl.ds(pl.multiple_of(core * rows + h * batch, batch), batch)
        for s in range(2):
            inside = slice(s * half + q * quarter, s * half + (q + 1) * quarter)
            at = pl.ds(pl.multiple_of(owner * block + s * half + q * quarter, quarter), quarter)
            value = middle[of_batch(h), at] + factor(owner, 1, inside) * total[:, s * quarter : (s + 1) * quarter]
            result_ref[at_rows, at] = value.astype(jnp.bfloat16)
            finals.append(copy(result_ref.at[at_rows, at], result_ref.at[at_rows, at], tp_name, near, "spread", final))
            start(finals[-1])

    n = 0
    for turn in DOWN_ORDER:
        if turn is None:
            up_rows(1)
            continue
        h, k = turn
        owner, q, j = owners[k]
        if j is not None and h == 0:
            serve()
            landed((range(8, 10), range(10, UNITS))[q], (j,))
        matrix = [
            down_all[pl.ds(pl.multiple_of(owner * block + s * half + q * quarter, quarter), quarter), :] for s in range(2)
        ]
        product = contract_last(active[h * rows : (h + 1) * rows, :], jnp.concatenate(matrix, axis=0))
        parts[1, k, h * rows : (h + 1) * rows, :] = product.astype(jnp.bfloat16)
        away = pl.ds(pl.multiple_of(h * rows + (1 - core) * batch, batch), batch)
        down_near.append(copy(parts.at[1, k, away, :], near_parts.at[1, k, of_batch(h), :], tp_name, near, "reduce"))
        start(down_near[n])
        if n >= 1:
            pair_down(n - 1)
        if n >= LAG:
            finish(n - LAG)
        n += 1
    pair_down(n - 1)
    for m in range(n - LAG, n):
        finish(m)
    serve()
    wait_all(finals)
    drain(common_sent)
    pl.when(inner == 0)(lambda: drain(edge_sent))
    pl.when(inner == 1)(lambda: drain(inner_sent))


def fused_body(
    tokens, first_gain, in_matrix, in_scale, conv_taps, decay_rate, recall_maps, admit_maps,
    out_matrix, out_scale, second_gain, up_matrix, up_scale, down_matrix, down_scale,
):
    length, model = tokens.shape[1:]
    width, hidden = in_matrix.shape[1], up_matrix.shape[1]
    fs = lax.axis_size("fs")
    block, step = model // fs, 256
    directions = decay_rate.shape[0]
    plane = pltpu.VMEM((directions, width // LANES, SEGMENTS * (length // SEGMENTS + GAP), LANES), jnp.float32)
    gate = pltpu.VMEM(recall_maps.shape, jnp.float32)
    pieces = pltpu.VMEM((2, model // step, length // 2, step), jnp.bfloat16)
    rows = pltpu.VMEM((length, model), jnp.bfloat16)
    channels = pltpu.VMEM((length, width), jnp.bfloat16)
    vmem, hbm = pl.BlockSpec(memory_space=pltpu.VMEM), pl.BlockSpec(memory_space=pl.ANY)
    arrived = UNITS * 3 + 27 + 7 * (model // step)
    result = pl.pallas_call(
        functools.partial(layer_kernel, ("rep", "fs", "tp")),
        out_shape=pltpu.VMEM((length, model), jnp.bfloat16),
        in_specs=[hbm] * 15,
        out_specs=vmem,
        scratch_shapes=[
            pltpu.VMEM((1, model), jnp.float32),
            pltpu.VMEM((1, width), jnp.float32),
            pltpu.VMEM(conv_taps.shape, jnp.float32),
            pltpu.VMEM(decay_rate.shape, jnp.float32),
            pltpu.VMEM((1, model), jnp.float32),
            pltpu.VMEM((1, hidden), jnp.float32),
            rows,
            pltpu.VMEM((block, width), jnp.float32),
            pltpu.VMEM((block, width), jnp.float32),
            pltpu.VMEM((block, hidden), jnp.float32),
            pltpu.VMEM((block, hidden), jnp.float32),
            gate, gate,
            pltpu.VMEM((model, width), jnp.bfloat16),
            pltpu.VMEM((model, width), jnp.bfloat16),
            pltpu.VMEM((model, hidden), jnp.bfloat16),
            pltpu.VMEM((model, hidden), jnp.bfloat16),
            pltpu.VMEM((fs, 2, block), jnp.float32),
            rows, rows, channels, rows,
            pltpu.VMEM((length + 2 * PAD, width), jnp.float32),
            plane, plane, plane,
            channels,
            pltpu.VMEM((length, hidden), jnp.bfloat16),
            pltpu.VMEM((2, model // step, length, step), jnp.bfloat16),
            pieces, pieces, pieces,
            pltpu.VMEM((length // 2, model), jnp.float32),
            pltpu.SemaphoreType.DMA((15,)),
            pltpu.SemaphoreType.DMA((17,)),
            pltpu.SemaphoreType.DMA((arrived,)),
        ],
        compiler_params=pltpu.CompilerParams(
            collective_id=0, has_side_effects=True, vmem_limit_bytes=59 * 2**20
        ),
        name="layer",
    )(
        tokens.reshape(length, model), first_gain[None], in_matrix, in_scale[None], conv_taps, decay_rate,
        recall_maps, admit_maps, out_matrix, out_scale[None], second_gain[None], up_matrix, up_scale[None], down_matrix,
        down_scale[None],
    )
    return result.reshape(tokens.shape)


def solution(mesh):
    placed = (
        P(("rep", "fs"), None, None),
        P(),
        P("fs", "tp"),
        P("tp"),
        P(None, "tp"),
        P(None, "tp"),
        P(None, "tp", None, None),
        P(None, "tp", None, None),
        P("fs", "tp"),
        P("fs"),
        P(),
        P("fs", "tp"),
        P("tp"),
        P("fs", "tp"),
        P("fs"),
    )
    small = (mesh.shape["rep"], mesh.shape["fs"], mesh.shape["tp"]) == (2, 4, 4)
    return jax.shard_map(
        fused_body if small else body, mesh=mesh, in_specs=placed, out_specs=P(("rep", "fs"), None, None), check_vma=False
    )
```

```python
import functools
import math
import jax
import jax.numpy as jnp
from jax import lax
from jax.experimental import pallas as pl
from jax.experimental.pallas import tpu as pltpu
from jax.sharding import PartitionSpec as P

EPSILON = 1e-06
RATE_GAIN = 8.0
LANES = 128
SEGMENTS = 8
PAD = 8
GAP = 8


def normalize(stream, gain):
    return stream * lax.rsqrt(jnp.mean(stream * stream, axis=-1, keepdims=True) + EPSILON) * gain


def one_minus_exp(y):
    series = 1.0 + y * (1.0 / 6.0)
    for k in (5.0, 4.0, 3.0, 2.0):
        series = 1.0 + y * (1.0 / k) * series
    return jnp.where(y > -0.25, -y * series, 1.0 - jnp.exp(y))


def sigmoid(x):
    return 0.5 * jnp.tanh(0.5 * x) + 0.5


def gate_part(padded, taps_ref, rate_ref, recall_ref, admit_ref, decay, drive, length, serve=None):
    directions, groups, block, _ = recall_ref.shape
    taps = taps_ref.shape[0]
    rows = length // SEGMENTS
    pitch = decay.shape[2] // SEGMENTS

    def tile_step(tile, _):
        base = pl.multiple_of(tile * rows, rows)
        into = pl.multiple_of(tile * pitch, 8)
        conv = jnp.zeros((rows, padded.shape[1]), jnp.float32)
        window = padded[pl.ds(base, rows + 2 * PAD), :]
        for k in range(taps):
            first = PAD - taps // 2 + k
            conv = conv + taps_ref[k : k + 1, :] * window[first : first + rows, :]
        narrow = conv.astype(jnp.bfloat16)
        for g in range(groups):
            values = conv[:, g * block : (g + 1) * block]
            left = narrow[:, g * block : (g + 1) * block]
            for d in range(directions):
                recall = sigmoid(jnp.dot(left, recall_ref[d, g].astype(jnp.bfloat16), preferred_element_type=jnp.float32))
                admit = sigmoid(jnp.dot(left, admit_ref[d, g].astype(jnp.bfloat16), preferred_element_type=jnp.float32))
                log_decay = recall * (-RATE_GAIN * rate_ref[d : d + 1, g * block : (g + 1) * block])
                a = jnp.exp(log_decay)
                b = jnp.sqrt(one_minus_exp(2.0 * log_decay)) * admit * values
                for c in range(block // LANES):
                    where = g * (block // LANES) + c
                    decay[d, where, pl.ds(into, rows), :] = a[:, c * LANES : (c + 1) * LANES]
                    drive[d, where, pl.ds(into, rows), :] = b[:, c * LANES : (c + 1) * LANES]
        return 0

    if serve is None:
        lax.fori_loop(0, SEGMENTS, tile_step, 0)
        return
    for first in range(0, SEGMENTS, 2):
        lax.fori_loop(first, first + 2, tile_step, 0)
        serve()


def scan_part(decay, drive, prefix, mixed_ref, length, serve=None):
    directions, chunks = decay.shape[:2]
    steps = length // SEGMENTS
    pitch = decay.shape[2] // SEGMENTS
    lanes = [(d, c) for d in range(directions) for c in range(chunks)]

    def scan_step(s, carried):
        out = []
        for (d, c), (state, product) in zip(lanes, carried):
            at = s if d == 0 else steps - 1 - s
            a = decay[d, c, pl.ds(at, SEGMENTS, stride=pitch), :]
            b = drive[d, c, pl.ds(at, SEGMENTS, stride=pitch), :]
            state = a * state + b
            product = a * product
            drive[d, c, pl.ds(at, SEGMENTS, stride=pitch), :] = state
            prefix[d, c, pl.ds(at, SEGMENTS, stride=pitch), :] = product
            out.append((state, product))
        return tuple(out)

    start = tuple((jnp.zeros((SEGMENTS, LANES), jnp.float32), jnp.ones((SEGMENTS, LANES), jnp.float32)) for _ in lanes)
    if serve is None:
        ends = lax.fori_loop(0, steps, scan_step, start, unroll=4)
    else:
        ends = start
        for first in range(0, steps, steps // 4):
            ends = lax.fori_loop(first, first + steps // 4, scan_step, ends, unroll=4)
            serve()
    ends = dict(zip(lanes, ends))

    for c in range(chunks):
        carries = []
        for d in range(directions):
            state, product = ends[(d, c)]
            order = range(SEGMENTS) if d == 0 else range(SEGMENTS - 1, -1, -1)
            carry = jnp.zeros((1, LANES), jnp.float32)
            entering = {}
            for k in order:
                entering[k] = carry
                carry = product[k : k + 1, :] * carry + state[k : k + 1, :]
            carries.append(entering)
        for k in range(SEGMENTS):
            span = pl.ds(k * pitch, steps)
            total = drive[0, c, span, :] + prefix[0, c, span, :] * carries[0][k]
            total = total + (drive[1, c, span, :] + prefix[1, c, span, :] * carries[1][k])
            mixed_ref[pl.ds(k * steps, steps), c * LANES : (c + 1) * LANES] = total.astype(jnp.bfloat16)
        if serve is not None:
            serve()


def recurrence_kernel(before_ref, taps_ref, rate_ref, recall_ref, admit_ref, mixed_ref, padded, decay, drive, prefix):
    length, width = before_ref.shape
    edge = jnp.zeros((PAD, width), jnp.float32)
    padded[pl.ds(0, PAD), :] = edge
    padded[pl.ds(PAD + length, PAD), :] = edge
    padded[pl.ds(PAD, length), :] = before_ref[...].astype(jnp.float32)
    gate_part(padded, taps_ref, rate_ref, recall_ref, admit_ref, decay, drive, length)
    scan_part(decay, drive, prefix, mixed_ref, length)


def recurrence(before, taps, rates, recall_maps, admit_maps):
    length, width = before.shape
    directions = rates.shape[0]
    chunks = width // LANES
    plane = pltpu.VMEM((directions, chunks, length, LANES), jnp.float32)
    return pl.pallas_call(
        recurrence_kernel,
        out_shape=jax.ShapeDtypeStruct((length, width), jnp.bfloat16),
        in_specs=[pl.BlockSpec(memory_space=pltpu.VMEM)] * 5,
        out_specs=pl.BlockSpec(memory_space=pltpu.VMEM),
        scratch_shapes=[pltpu.VMEM((length + 2 * PAD, width), jnp.float32), plane, plane, plane],
        compiler_params=pltpu.CompilerParams(vmem_limit_bytes=24 * 2**20),
        cost_estimate=pl.CostEstimate(flops=16 * length * width * 256, bytes_accessed=8 * 2**20, transcendentals=8 * length * width),
        name="recurrence",
    )(before, taps, rates, recall_maps, admit_maps)


def contract_last(left, right):
    return lax.dot_general(
        left, right, (((1,), (1,)), ((), ())), preferred_element_type=jnp.float32
    )


def gather(shard):
    copies = lax.axis_size("rep")
    if shard.shape[0] % (16 * copies):
        return lax.all_gather(shard.astype(jnp.bfloat16), "fs", axis=0, tiled=True)
    rows = shard.shape[0] // copies
    part = lax.dynamic_slice_in_dim(shard, lax.axis_index("rep") * rows, rows, 0)
    return lax.all_gather(part.astype(jnp.bfloat16), ("fs", "rep"), axis=0, tiled=True)


def body(
    tokens,
    first_gain,
    in_matrix,
    in_scale,
    conv_taps,
    decay_rate,
    recall_maps,
    admit_maps,
    out_matrix,
    out_scale,
    second_gain,
    up_matrix,
    up_scale,
    down_matrix,
    down_scale,
):
    stream = tokens.reshape(tokens.shape[1], tokens.shape[2]).astype(jnp.float32)
    factors = lax.all_gather(
        jnp.stack([out_scale, down_scale]).astype(jnp.bfloat16), "fs", axis=1, tiled=True
    )
    in_cols = gather(in_matrix)
    normed = normalize(stream, first_gain).astype(jnp.bfloat16)
    before = (
        jnp.dot(normed, in_cols, preferred_element_type=jnp.float32) * in_scale.astype(jnp.bfloat16)
    ).astype(jnp.bfloat16)
    mixed = recurrence(before, conv_taps, decay_rate, recall_maps, admit_maps)
    partial_value = contract_last(mixed, gather(out_matrix))
    middle = stream + factors[0] * lax.psum(partial_value.astype(jnp.bfloat16), "tp").astype(
        jnp.float32
    )
    second_normed = normalize(middle, second_gain).astype(jnp.bfloat16)
    raised = jnp.dot(second_normed, gather(up_matrix), preferred_element_type=jnp.float32)
    active = jnp.square(jax.nn.relu(raised * up_scale.astype(jnp.bfloat16))).astype(jnp.bfloat16)
    lowered = contract_last(active, gather(down_matrix))
    result = (
        middle + factors[1] * lax.psum(lowered.astype(jnp.bfloat16), "tp").astype(jnp.float32)
    ).astype(jnp.bfloat16)
    return result.reshape(tokens.shape)

MESH = pl.DeviceIdType.MESH
UNITS = 20
SPLIT = 2
OWN_TO_MATE = (2, 3, 4, 5, 6, 7, 8, 9, 10, 11, 12, 13, 14)
OWN_TO_MATE_AFTER = {8: (15,), 15: (16, 17), 16: (18, 19)}
OWN_TO_OTHER = (0, 1, 2)
OWN_TO_OTHER_AFTER = {1: (3, 4), 2: (5, 6), 3: (7,), 4: (8,), 5: (9,), 8: (10, 11, 12), 12: (13, 14, 15, 16), 15: (17,), 16: (18, 19)}
EDGE_SENDS = ((1, 2), (1, 3), (0, 2), (0, 3), (1, 4), (1, 5), (1, 6), (1, 7), (1, 8), (1, 9), (1, 10), (1, 11), (0, 4), (0, 5), (0, 6), (0, 7), (0, 8), (0, 9), (0, 10), (0, 11), (1, 12), (1, 13), (1, 14), (1, 15), (1, 16), (1, 17), (1, 18), (1, 19), (0, 12), (0, 13), (0, 14), (0, 15), (0, 16), (0, 17), (0, 18), (0, 19))
DOWN_ORDER = ((0, 0), (0, 1), (0, 2), (0, 3), None, (1, 0), (1, 1), (1, 2), (1, 3), (0, 4), (1, 4), (0, 5), (1, 5), (0, 6), (1, 6), (0, 7), (1, 7))
LAG = 4
EDGE_SERVES = (
    (2, 3, 4, 5, 6, 7, 8, 9, 10, 11, 12, 13, 14, 22, 23, 24, 42),
    (25,),
    (),
    (26,),
    (),
    (43,),
    (),
    (27,),
    (),
    (44,),
    (),
    (28,),
    (),
    (),
    (),
    (45,),
    (),
    (),
    (),
    (29,),
    (),
    (),
    (46, 47),
    (),
    (),
    (48,),
    (15,),
    (30,),
    (31,),
    (32,),
    (49,),
    (50,),
    (51, 52),
    (),
    (),
    (),
    (33, 34),
    (),
    (35,),
    (),
    (),
    (),
    (),
    (),
    (36,),
    (53,),
    (54,),
    (55, 16),
    (),
    (),
    (),
    (17,),
    (),
    (),
    (),
    (37,),
    (),
    (),
    (),
    (),
    (),
    (56,),
    (),
    (),
    (18,),
    (),
    (19,),
    (),
    (),
    (38,),
    (),
    (39,),
    (57,),
    (),
    (),
    (58,),
    (),
    (59,),
    (),
    (),
    (),
    (),
    (),
    (),
    (),
    (),
    (),
    (),
    (),
    (),
    (),
    (),
    (),
)
INNER_SERVES = (
    (),
    (),
    (),
    (),
    (0, 20, 1, 21),
    (22, 40),
    (41,),
    (23,),
    (),
    (),
    (24,),
    (2,),
    (3, 42),
    (),
    (25,),
    (),
    (),
    (26,),
    (),
    (4, 43),
    (5,),
    (27, 6),
    (),
    (7, 44),
    (8,),
    (28,),
    (),
    (9,),
    (45,),
    (),
    (),
    (10,),
    (29,),
    (),
    (),
    (11, 46),
    (),
    (),
    (47, 48),
    (),
    (),
    (30,),
    (31,),
    (32,),
    (49,),
    (50,),
    (51,),
    (12,),
    (13, 14),
    (),
    (52,),
    (),
    (15, 33),
    (),
    (16,),
    (),
    (),
    (),
    (),
    (34, 17, 35),
    (18, 36),
    (19, 53),
    (54,),
    (55,),
    (37,),
    (),
    (),
    (56,),
    (),
    (),
    (38,),
    (),
    (),
    (),
    (),
    (),
    (),
    (39,),
    (),
    (),
    (57,),
    (58,),
    (),
    (),
    (),
    (59,),
    (),
    (),
    (),
    (),
    (),
    (),
    (),
    (),
    (),
    (),
    (),
    (),
    (),
    (),
    (),
    (),
    (),
    (),
    (),
    (),
    (),
    (),
    (),
)


def layer_kernel(
    names, tokens_hbm, first_hbm, in_hbm, in_scale_hbm, taps_hbm, rate_hbm, recall_hbm, admit_hbm,
    out_hbm, out_scale_hbm, second_hbm, up_hbm, up_scale_hbm, down_hbm, down_scale_hbm,
    result_ref,
    first_ref, in_scale_ref, taps_ref, rate_ref, second_ref, up_scale_ref, tokens, in_own, out_own, up_own, down_own, recall_ref, admit_ref,
    in_all, out_all, up_all, down_all, scales_all, normed, guest, before, second_normed, padded, decay, drive, prefix,
    mixed, active, parts, near_parts, pairs, far_pairs, middle, load, send, recv,
):
    replica, place, rank = (lax.axis_index(name) for name in names)
    rep_name, fs_name, tp_name = names
    fs = 4
    length, model = tokens.shape
    block = model // fs
    half, quarter = block // 2, block // 4
    mate = place + 1 - 2 * lax.rem(place, 2)
    inner = lax.rem(lax.div(place + 1, 2), 2)
    other = fs - 1 - place
    other_mate = fs - 1 - mate
    slots = (mate, inner * other + (1 - inner) * other_mate, inner * other_mate + (1 - inner) * other)
    core = lax.rem(rank, 2)
    near = rank + 1 - 2 * core
    far = lax.rem(rank + 2, 4)
    recvs, groups = [0], {}

    def fresh():
        recvs[0] += 1
        return recvs[0] - 1

    def whole_copy(src, dst, axis, peer, group, into):
        return pltpu.make_async_remote_copy(
            src_ref=src, dst_ref=dst, send_sem=send.at[groups.setdefault(group, len(groups))], recv_sem=recv.at[into],
            device_id={axis: peer}, device_id_type=MESH,
        )

    def bytes_of(ref):
        return math.prod(ref.shape) * jnp.dtype(ref.dtype).itemsize

    def waiter(size, group, into):
        count = size // bytes_of(up_all.at[0])
        return whole_copy(up_all.at[0:count, :], up_all.at[0:count, :], tp_name, near, group, into)

    class copy:
        def __init__(self, src, dst, axis, peer, group, into=None):
            self.into = fresh() if into is None else into
            self.group, self.size = group, bytes_of(src)
            self.one = whole_copy(src, dst, axis, peer, group, self.into)
            self.start, self.wait_recv, self.wait_send = self.one.start, self.one.wait_recv, self.one.wait_send

    common_sent, edge_sent, inner_sent = {}, {}, {}

    def start(one, sent=common_sent):
        one.start()
        sent.setdefault(one.group, []).append(one)

    def drain(sent):
        for group, copies in sent.items():
            if len(copies) == 1:
                copies[0].wait_send()
            else:
                waiter(sum(one.size for one in copies), group, copies[0].into).wait_send()

    def wait_all(copies):
        waiter(sum(one.size for one in copies), copies[0].group, copies[0].into).wait_recv()

    barrier = pltpu.get_barrier_semaphore()
    greeted = [(rep_name, 1 - replica)]
    greeted += [(fs_name, mate), (tp_name, near), (tp_name, far)]

    def greet(axis, peer):
        pl.semaphore_signal(barrier, inc=1, device_id={axis: peer}, device_id_type=MESH)

    for axis, peer in greeted:
        greet(axis, peer)
    pl.when(inner == 1)(lambda: greet(fs_name, other))

    loads = [
        pltpu.make_async_copy(src, dst, load.at[i])
        for i, (src, dst) in enumerate((
            (in_hbm, in_own), (out_hbm, out_own), (first_hbm, first_ref), (tokens_hbm, tokens), (up_hbm, up_own),
            (down_hbm, down_own), (out_scale_hbm, scales_all.at[place, 0:1, :]), (down_scale_hbm, scales_all.at[place, 1:2, :]),
            (in_scale_hbm, in_scale_ref), (taps_hbm, taps_ref), (rate_hbm, rate_ref), (second_hbm, second_ref),
            (up_scale_hbm, up_scale_ref), (recall_hbm, recall_ref), (admit_hbm, admit_ref),
        ))
    ]
    for one in loads:
        one.start()
    load_in, load_out, load_first, load_tokens, load_up, load_down = loads[:6]
    load_scales, load_rest = loads[6:8], loads[8:]

    own_rows = pl.ds(pl.multiple_of(place * block, block), block)
    load_in.wait()
    in_all[own_rows, :] = in_own[...].astype(jnp.bfloat16)
    load_out.wait()
    out_all[own_rows, :] = out_own[...].astype(jnp.bfloat16)

    wide = up_all.shape[1] // 2

    def view(owner, unit, side):
        def rows(first, count):
            return pl.ds(pl.multiple_of(owner * block + side * half + first, count), count)

        def columns(part):
            return slice(part * wide, (part + 1) * wide)

        if unit < 4:
            return (in_all, out_all)[unit // 2].at[rows(unit % 2 * quarter, quarter), :]
        eighth = quarter // 2
        if unit < 12:
            return up_all.at[rows((unit - 4) % 4 * eighth, eighth), columns((unit - 4) // 4)]
        return down_all.at[rows((unit - 12) // 4 * quarter + unit % 2 * eighth, eighth), columns((unit - 12) % 4 // 2)]

    to_mate, extra, to_other, pass_mate, pass_other, pass_last, swaps = [], [], [], [], [], [], []
    bundles = [(0, 1), (2, 3)] + [tuple(range(i, i + 4)) for i in range(4, UNITS, 4)]
    landings = {}
    for bundle in bundles:
        shared = [fresh() for _ in range(3 if bundle[0] >= 12 else 1)] * (1 if bundle[0] >= 12 else 3)
        for unit in bundle:
            landings[unit] = shared
    for unit in range(UNITS):
        into = [fresh() for _ in range(3)]
        own, first, second, third = (view(owner, unit, replica) for owner in (place,) + slots)
        rest = view(place, unit, 1 - replica)
        land = landings[unit]
        to_mate.append(copy(own, own, fs_name, mate, "to_mate", into[0]))
        extra.append(copy(rest, rest, fs_name, mate, "extra", land[0]) if unit >= SPLIT else None)
        to_other.append(copy(own, own, fs_name, other, "to_other", into[1]))
        pass_mate.append(copy(first, first, fs_name, other, "pass_mate", into[2]))
        pass_other.append(copy(second, second, fs_name, mate, "pass_other", into[1]) if unit >= SPLIT else None)
        pass_last.append(copy(third, third, fs_name, mate, "pass_last", into[2]))
        swaps.append([copy(part, part, rep_name, 1 - replica, f"swap{j}", land[j]) for j, part in enumerate((first, second, third))])
    arrivals = (to_mate, to_other, pass_last)

    def serve_edge(codes):
        for code in codes:
            slot, unit = code // UNITS, code % UNITS
            arrivals[slot][unit].wait_recv()
            start(swaps[unit][slot], edge_sent)

    def serve_inner(codes):
        for code in codes:
            slot, unit = code // UNITS, code % UNITS
            arrivals[slot][unit].wait_recv()
            if slot or unit < SPLIT:
                start(swaps[unit][slot], inner_sent)
            if slot == 0:
                start(pass_mate[unit], inner_sent)
                for u in OWN_TO_OTHER_AFTER.get(unit, ()):
                    start(to_other[u], inner_sent)
            elif unit >= SPLIT:
                start((pass_other, pass_last)[slot - 1][unit], inner_sent)
            if slot == 2:
                for u in OWN_TO_MATE_AFTER.get(unit, ()):
                    start(to_mate[u], inner_sent)

    points = {"edge": 0, "inner": 0}

    def edge_next():
        points["edge"] += 1
        return EDGE_SERVES[points["edge"] - 1]

    def inner_next():
        points["inner"] += 1
        return INNER_SERVES[points["inner"] - 1]

    def serve():
        edge_codes, inner_codes = edge_next(), inner_next()
        if edge_codes:
            pl.when(inner == 0)(lambda: serve_edge(edge_codes))
        if inner_codes:
            pl.when(inner == 1)(lambda: serve_inner(inner_codes))

    def landed(units, taken=(0, 1, 2)):
        wait_all([swaps[unit][slot] for unit in units for slot in taken])

    piece = 32
    pieces = length // 4 // piece

    def guest_rows(owner, i):
        return pl.ds(pl.multiple_of(owner * (length // 4) + i * piece, piece), piece)

    tok, tok_far, tok_near, tok_onward = [], [], [], []
    guest_near = fresh()
    for i in range(pieces):
        mine, theirs = guest_rows(rank, i), guest_rows(far, i)
        tok.append(copy(normed.at[mine, :], guest.at[mine, :], fs_name, mate, "guest"))
        tok_far.append(copy(guest.at[mine, :], guest.at[mine, :], tp_name, far, "guest"))
        tok_near.append(copy(guest.at[mine, :], guest.at[mine, :], tp_name, near, "guest", guest_near))
        tok_onward.append(copy(guest.at[theirs, :], guest.at[theirs, :], tp_name, near, "guest", guest_near))
    step = 256
    tiles = [slice(i * step, (i + 1) * step) for i in range(in_all.shape[1] // step)]
    given_before = [copy(before.at[:, at], before.at[:, at], fs_name, mate, "guest") for at in tiles]

    pl.when(inner == 0)(lambda: pl.semaphore_wait(barrier, len(greeted)))
    pl.when(inner == 1)(lambda: pl.semaphore_wait(barrier, len(greeted) + 1))

    @pl.when(inner == 0)
    def _():
        for unit in range(SPLIT):
            start(to_mate[unit], edge_sent)

    @pl.when(inner == 1)
    def _():
        for unit in OWN_TO_OTHER:
            start(to_other[unit], inner_sent)
        for unit in OWN_TO_MATE:
            if unit < 4:
                start(to_mate[unit], inner_sent)

    def norm_rows(at):
        normed[at, :] = normalize(tokens[at, :].astype(jnp.float32), first_ref[...]).astype(jnp.bfloat16)

    load_first.wait()
    load_tokens.wait()

    @pl.when(inner == 0)
    def _():
        for i in range(pieces):
            norm_rows(guest_rows(rank, i))
            start(tok[i], edge_sent)

    load_up.wait()
    up_all[own_rows, :] = up_own[...].astype(jnp.bfloat16)
    load_down.wait()
    down_all[own_rows, :] = down_own[...].astype(jnp.bfloat16)
    for one in load_scales:
        one.wait()
    into = [fresh() for _ in range(3)]
    own, first, second, third = (scales_all.at[owner] for owner in (place,) + slots)
    scale_in = [
        copy(own, own, fs_name, mate, "scale0", into[0]), copy(own, own, fs_name, other, "scale1", into[1]),
        copy(third, third, fs_name, mate, "scale2", into[2]),
    ]
    scale_out = [
        copy(first, first, fs_name, other, "scale3", into[2]), copy(second, second, fs_name, mate, "scale4", into[1]), scale_in[2],
    ]
    start(scale_in[0])
    pl.when(inner == 1)(lambda: start(scale_in[1], inner_sent))

    def pass_scales(slot):
        scale_in[slot].wait_recv()
        start(scale_out[slot], inner_sent)

    for one in load_rest:
        one.wait()
    edge = jnp.zeros((PAD, padded.shape[1]), jnp.float32)
    padded[pl.ds(0, PAD), :] = edge
    padded[pl.ds(PAD + length, PAD), :] = edge

    @pl.when(inner == 0)
    def _():
        for whole, unit in EDGE_SENDS:
            start((to_mate if whole else extra)[unit], edge_sent)
        serve_edge(edge_next())
        for one, at in zip(given_before, tiles):
            one.wait_recv()
            padded[pl.ds(PAD, length), at] = before[:, at].astype(jnp.float32)

    @pl.when(inner == 1)
    def _():
        for unit in OWN_TO_MATE:
            if unit >= 4:
                start(to_mate[unit], inner_sent)
        tile = 64
        for i in range(4):

            def norm_step(k, _, i=i):
                norm_rows(pl.ds(pl.multiple_of((2 * i + k) * tile, tile), tile))
                return 0

            lax.fori_loop(0, length // tile // 4, norm_step, 0)
            serve_inner(inner_next())
        for i in range(pieces):
            serve_inner(inner_next())
            tok[i].wait_recv()
            start(tok_far[i], inner_sent)
            start(tok_near[i], inner_sent)
        pass_scales(0)
        pass_scales(1)
        for i in range(pieces):
            serve_inner(inner_next())
            tok_far[i].wait_recv()
            start(tok_onward[i], inner_sent)
        serve_inner(inner_next())
        landed(range(SPLIT))
        wait_all(tok_near + tok_onward)

        def project_in(values, at):
            product = jnp.dot(values[...], in_all[:, at], preferred_element_type=jnp.float32)
            return (product * in_scale_ref[:, at].astype(jnp.bfloat16).astype(jnp.float32)).astype(jnp.bfloat16)

        for one, at in zip(given_before, tiles):
            before[:, at] = project_in(guest, at)
            start(one, inner_sent)
            serve_inner(inner_next())
        pass_scales(2)
        for at in tiles:
            padded[pl.ds(PAD, length), at] = project_in(normed, at).astype(jnp.float32)
            serve_inner(inner_next())

    gate_part(padded, taps_ref, rate_ref, recall_ref, admit_ref, decay, drive, length, serve)
    scan_part(decay, drive, prefix, mixed, length, serve)

    serve()
    landed((2, 3))

    @pl.when(inner == 0)
    def _():
        for one in scale_in:
            one.wait_recv()

    chunks = model // step
    rows = length // 2
    batch = rows // 2
    kept = pl.ds(pl.multiple_of(core * rows, rows), rows)
    given = pl.ds(pl.multiple_of((1 - core) * rows, rows), rows)

    def of_batch(h):
        return slice(h * batch, (h + 1) * batch)

    def factor(owner, which, at):
        return scales_all[owner, which : which + 1, at].astype(jnp.bfloat16).astype(jnp.float32)

    to_near = [copy(parts.at[0, k, given, :], near_parts.at[0, k], tp_name, near, "reduce") for k in range(chunks)]
    to_far = [
        [
            [copy(pairs.at[stage, k, of_batch(h), :], far_pairs.at[stage, k, of_batch(h), :], tp_name, far, "reduce") for k in range(chunks)]
            for h in range(2)
        ]
        for stage in range(2)
    ]

    def far_total(stage, h, k):
        to_far[stage][h][k].wait_recv()
        return pairs[stage, k, of_batch(h), :].astype(jnp.float32) + far_pairs[stage, k, of_batch(h), :].astype(jnp.float32)

    for k in range(chunks + 2):
        if k < chunks:
            product = contract_last(mixed[...], out_all[k * step : (k + 1) * step, :])
            parts[0, k] = product.astype(jnp.bfloat16)
            start(to_near[k])
        serve()
        if k >= 2:
            to_near[k - 2].wait_recv()
            total = parts[0, k - 2, kept, :].astype(jnp.float32) + near_parts[0, k - 2].astype(jnp.float32)
            pairs[0, k - 2] = total.astype(jnp.bfloat16)
            start(to_far[0][0][k - 2])
    for k in range(chunks):
        start(to_far[0][1][k])

    spreads = []

    def middle_rows(h):
        squares = jnp.zeros((batch, 1), jnp.float32)
        at_rows = pl.ds(pl.multiple_of(core * rows + h * batch, batch), batch)
        for k in range(chunks):
            serve()
            at = slice(k * step, (k + 1) * step)
            inside = slice(k * step % block, k * step % block + step)
            value = tokens[at_rows, at].astype(jnp.float32) + factor(k * step // block, 0, inside) * far_total(0, h, k)
            middle[of_batch(h), at] = value
            squares = squares + jnp.sum(value * value, axis=1, keepdims=True)
        inverse = lax.rsqrt(squares * (1.0 / model) + EPSILON)
        at = pl.ds(pl.multiple_of(h * rows + core * batch, batch), batch)
        second_normed[at, :] = (middle[of_batch(h), :] * inverse * second_ref[...]).astype(jnp.bfloat16)
        spreads.append(copy(second_normed.at[at, :], second_normed.at[at, :], tp_name, near, "spread"))
        start(spreads[h])

    def up_rows(h):
        serve()
        spreads[h].wait_recv()
        at_rows = slice(h * rows, (h + 1) * rows)
        for part in range(2):
            serve()
            if h == 0:
                landed(bundles[2 + part])
            for i in range(part * (wide // step), (part + 1) * (wide // step)):
                at = slice(i * step, (i + 1) * step)
                raised = jnp.dot(second_normed[at_rows, :], up_all[:, at], preferred_element_type=jnp.float32)
                raised = raised * up_scale_ref[:, at].astype(jnp.bfloat16).astype(jnp.float32)
                active[at_rows, at] = jnp.square(jnp.maximum(raised, 0.0)).astype(jnp.bfloat16)
                serve()

    middle_rows(0)
    up_rows(0)
    middle_rows(1)

    owners = [(place, 0, None), (place, 1, None)] + [(slots[j], q, j) for q in range(2) for j in range(3)]
    turns = [turn for turn in DOWN_ORDER if turn is not None]
    down_near, finals, final = [], [], fresh()

    def pair_down(n):
        h, k = turns[n]
        serve()
        down_near[n].wait_recv()
        at = pl.ds(pl.multiple_of(h * rows + core * batch, batch), batch)
        total = parts[1, k, at, :].astype(jnp.float32) + near_parts[1, k, of_batch(h), :].astype(jnp.float32)
        pairs[1, k, of_batch(h), :] = total.astype(jnp.bfloat16)
        start(to_far[1][h][k])

    def finish(n):
        h, k = turns[n]
        owner, q, _ = owners[k]
        serve()
        total = far_total(1, h, k)
        at_rows = pl.ds(pl.multiple_of(core * rows + h * batch, batch), batch)
        for s in range(2):
            inside = slice(s * half + q * quarter, s * half + (q + 1) * quarter)
            at = pl.ds(pl.multiple_of(owner * block + s * half + q * quarter, quarter), quarter)
            value = middle[of_batch(h), at] + factor(owner, 1, inside) * total[:, s * quarter : (s + 1) * quarter]
            result_ref[at_rows, at] = value.astype(jnp.bfloat16)
            finals.append(copy(result_ref.at[at_rows, at], result_ref.at[at_rows, at], tp_name, near, "spread", final))
            start(finals[-1])

    n = 0
    for turn in DOWN_ORDER:
        if turn is None:
            up_rows(1)
            continue
        h, k = turn
        owner, q, j = owners[k]
        if j is not None and h == 0:
            serve()
            landed(bundles[4 + q], (j,))
        matrix = [
            down_all[pl.ds(pl.multiple_of(owner * block + s * half + q * quarter, quarter), quarter), :] for s in range(2)
        ]
        product = contract_last(active[h * rows : (h + 1) * rows, :], jnp.concatenate(matrix, axis=0))
        parts[1, k, h * rows : (h + 1) * rows, :] = product.astype(jnp.bfloat16)
        away = pl.ds(pl.multiple_of(h * rows + (1 - core) * batch, batch), batch)
        down_near.append(copy(parts.at[1, k, away, :], near_parts.at[1, k, of_batch(h), :], tp_name, near, "reduce"))
        start(down_near[n])
        if n >= 1:
            pair_down(n - 1)
        if n >= LAG:
            finish(n - LAG)
        n += 1
    pair_down(n - 1)
    for m in range(n - LAG, n):
        finish(m)
    serve()
    wait_all(finals)
    drain(common_sent)
    pl.when(inner == 0)(lambda: drain(edge_sent))
    pl.when(inner == 1)(lambda: drain(inner_sent))


def fused_body(
    tokens, first_gain, in_matrix, in_scale, conv_taps, decay_rate, recall_maps, admit_maps,
    out_matrix, out_scale, second_gain, up_matrix, up_scale, down_matrix, down_scale,
):
    length, model = tokens.shape[1:]
    width, hidden = in_matrix.shape[1], up_matrix.shape[1]
    fs = lax.axis_size("fs")
    block, step = model // fs, 256
    directions = decay_rate.shape[0]
    plane = pltpu.VMEM((directions, width // LANES, SEGMENTS * (length // SEGMENTS + GAP), LANES), jnp.float32)
    gate = pltpu.VMEM(recall_maps.shape, jnp.float32)
    pieces = pltpu.VMEM((2, model // step, length // 2, step), jnp.bfloat16)
    rows = pltpu.VMEM((length, model), jnp.bfloat16)
    channels = pltpu.VMEM((length, width), jnp.bfloat16)
    vmem, hbm = pl.BlockSpec(memory_space=pltpu.VMEM), pl.BlockSpec(memory_space=pl.ANY)
    arrived = UNITS * 3 + 27 + 7 * (model // step)
    result = pl.pallas_call(
        functools.partial(layer_kernel, ("rep", "fs", "tp")),
        out_shape=pltpu.VMEM((length, model), jnp.bfloat16),
        in_specs=[hbm] * 15,
        out_specs=vmem,
        scratch_shapes=[
            pltpu.VMEM((1, model), jnp.float32),
            pltpu.VMEM((1, width), jnp.float32),
            pltpu.VMEM(conv_taps.shape, jnp.float32),
            pltpu.VMEM(decay_rate.shape, jnp.float32),
            pltpu.VMEM((1, model), jnp.float32),
            pltpu.VMEM((1, hidden), jnp.float32),
            rows,
            pltpu.VMEM((block, width), jnp.float32),
            pltpu.VMEM((block, width), jnp.float32),
            pltpu.VMEM((block, hidden), jnp.float32),
            pltpu.VMEM((block, hidden), jnp.float32),
            gate, gate,
            pltpu.VMEM((model, width), jnp.bfloat16),
            pltpu.VMEM((model, width), jnp.bfloat16),
            pltpu.VMEM((model, hidden), jnp.bfloat16),
            pltpu.VMEM((model, hidden), jnp.bfloat16),
            pltpu.VMEM((fs, 2, block), jnp.float32),
            rows, rows, channels, rows,
            pltpu.VMEM((length + 2 * PAD, width), jnp.float32),
            plane, plane, plane,
            channels,
            pltpu.VMEM((length, hidden), jnp.bfloat16),
            pltpu.VMEM((2, model // step, length, step), jnp.bfloat16),
            pieces, pieces, pieces,
            pltpu.VMEM((length // 2, model), jnp.float32),
            pltpu.SemaphoreType.DMA((15,)),
            pltpu.SemaphoreType.DMA((17,)),
            pltpu.SemaphoreType.DMA((arrived,)),
        ],
        compiler_params=pltpu.CompilerParams(
            collective_id=0, has_side_effects=True, vmem_limit_bytes=59 * 2**20
        ),
        name="layer",
    )(
        tokens.reshape(length, model), first_gain[None], in_matrix, in_scale[None], conv_taps, decay_rate,
        recall_maps, admit_maps, out_matrix, out_scale[None], second_gain[None], up_matrix, up_scale[None], down_matrix,
        down_scale[None],
    )
    return result.reshape(tokens.shape)


def solution(mesh):
    placed = (
        P(("rep", "fs"), None, None),
        P(),
        P("fs", "tp"),
        P("tp"),
        P(None, "tp"),
        P(None, "tp"),
        P(None, "tp", None, None),
        P(None, "tp", None, None),
        P("fs", "tp"),
        P("fs"),
        P(),
        P("fs", "tp"),
        P("tp"),
        P("fs", "tp"),
        P("fs"),
    )
    small = (mesh.shape["rep"], mesh.shape["fs"], mesh.shape["tp"]) == (2, 4, 4)
    return jax.shard_map(
        fused_body if small else body, mesh=mesh, in_specs=placed, out_specs=P(("rep", "fs"), None, None), check_vma=False
    )
```

```python
import functools
import math
import jax
import jax.numpy as jnp
from jax import lax
from jax.experimental import pallas as pl
from jax.experimental.pallas import tpu as pltpu
from jax.sharding import PartitionSpec as P

EPSILON = 1e-06
RATE_GAIN = 8.0
LANES = 128
SEGMENTS = 8
PAD = 8
GAP = 8


def normalize(stream, gain):
    return stream * lax.rsqrt(jnp.mean(stream * stream, axis=-1, keepdims=True) + EPSILON) * gain


def one_minus_exp(y):
    series = 1.0 + y * (1.0 / 6.0)
    for k in (5.0, 4.0, 3.0, 2.0):
        series = 1.0 + y * (1.0 / k) * series
    return jnp.where(y > -0.25, -y * series, 1.0 - jnp.exp(y))


def sigmoid(x):
    return 0.5 * jnp.tanh(0.5 * x) + 0.5


def gate_part(padded, taps_ref, rate_ref, recall_ref, admit_ref, decay, drive, length, serve=None):
    directions, groups, block, _ = recall_ref.shape
    taps = taps_ref.shape[0]
    rows = length // SEGMENTS
    pitch = decay.shape[2] // SEGMENTS

    def tile_step(tile, _):
        base = pl.multiple_of(tile * rows, rows)
        into = pl.multiple_of(tile * pitch, 8)
        conv = jnp.zeros((rows, padded.shape[1]), jnp.float32)
        window = padded[pl.ds(base, rows + 2 * PAD), :]
        for k in range(taps):
            first = PAD - taps // 2 + k
            conv = conv + taps_ref[k : k + 1, :] * window[first : first + rows, :]
        narrow = conv.astype(jnp.bfloat16)
        for g in range(groups):
            values = conv[:, g * block : (g + 1) * block]
            left = narrow[:, g * block : (g + 1) * block]
            for d in range(directions):
                recall = sigmoid(jnp.dot(left, recall_ref[d, g].astype(jnp.bfloat16), preferred_element_type=jnp.float32))
                admit = sigmoid(jnp.dot(left, admit_ref[d, g].astype(jnp.bfloat16), preferred_element_type=jnp.float32))
                log_decay = recall * (-RATE_GAIN * rate_ref[d : d + 1, g * block : (g + 1) * block])
                a = jnp.exp(log_decay)
                b = jnp.sqrt(one_minus_exp(2.0 * log_decay)) * admit * values
                for c in range(block // LANES):
                    where = g * (block // LANES) + c
                    decay[d, where, pl.ds(into, rows), :] = a[:, c * LANES : (c + 1) * LANES]
                    drive[d, where, pl.ds(into, rows), :] = b[:, c * LANES : (c + 1) * LANES]
        return 0

    if serve is None:
        lax.fori_loop(0, SEGMENTS, tile_step, 0)
        return
    for first in range(0, SEGMENTS, 2):
        lax.fori_loop(first, first + 2, tile_step, 0)
        serve()


def scan_part(decay, drive, prefix, mixed_ref, length, serve=None):
    directions, chunks = decay.shape[:2]
    steps = length // SEGMENTS
    pitch = decay.shape[2] // SEGMENTS
    lanes = [(d, c) for d in range(directions) for c in range(chunks)]

    def scan_step(s, carried):
        out = []
        for (d, c), (state, product) in zip(lanes, carried):
            at = s if d == 0 else steps - 1 - s
            a = decay[d, c, pl.ds(at, SEGMENTS, stride=pitch), :]
            b = drive[d, c, pl.ds(at, SEGMENTS, stride=pitch), :]
            state = a * state + b
            product = a * product
            drive[d, c, pl.ds(at, SEGMENTS, stride=pitch), :] = state
            prefix[d, c, pl.ds(at, SEGMENTS, stride=pitch), :] = product
            out.append((state, product))
        return tuple(out)

    start = tuple((jnp.zeros((SEGMENTS, LANES), jnp.float32), jnp.ones((SEGMENTS, LANES), jnp.float32)) for _ in lanes)
    if serve is None:
        ends = lax.fori_loop(0, steps, scan_step, start, unroll=4)
    else:
        ends = start
        for first in range(0, steps, steps // 4):
            ends = lax.fori_loop(first, first + steps // 4, scan_step, ends, unroll=4)
            serve()
    ends = dict(zip(lanes, ends))

    for c in range(chunks):
        carries = []
        for d in range(directions):
            state, product = ends[(d, c)]
            order = range(SEGMENTS) if d == 0 else range(SEGMENTS - 1, -1, -1)
            carry = jnp.zeros((1, LANES), jnp.float32)
            entering = {}
            for k in order:
                entering[k] = carry
                carry = product[k : k + 1, :] * carry + state[k : k + 1, :]
            carries.append(entering)
        for k in range(SEGMENTS):
            span = pl.ds(k * pitch, steps)
            total = drive[0, c, span, :] + prefix[0, c, span, :] * carries[0][k]
            total = total + (drive[1, c, span, :] + prefix[1, c, span, :] * carries[1][k])
            mixed_ref[pl.ds(k * steps, steps), c * LANES : (c + 1) * LANES] = total.astype(jnp.bfloat16)
        if serve is not None:
            serve()


def recurrence_kernel(before_ref, taps_ref, rate_ref, recall_ref, admit_ref, mixed_ref, padded, decay, drive, prefix):
    length, width = before_ref.shape
    edge = jnp.zeros((PAD, width), jnp.float32)
    padded[pl.ds(0, PAD), :] = edge
    padded[pl.ds(PAD + length, PAD), :] = edge
    padded[pl.ds(PAD, length), :] = before_ref[...].astype(jnp.float32)
    gate_part(padded, taps_ref, rate_ref, recall_ref, admit_ref, decay, drive, length)
    scan_part(decay, drive, prefix, mixed_ref, length)


def recurrence(before, taps, rates, recall_maps, admit_maps):
    length, width = before.shape
    directions = rates.shape[0]
    chunks = width // LANES
    plane = pltpu.VMEM((directions, chunks, length, LANES), jnp.float32)
    return pl.pallas_call(
        recurrence_kernel,
        out_shape=jax.ShapeDtypeStruct((length, width), jnp.bfloat16),
        in_specs=[pl.BlockSpec(memory_space=pltpu.VMEM)] * 5,
        out_specs=pl.BlockSpec(memory_space=pltpu.VMEM),
        scratch_shapes=[pltpu.VMEM((length + 2 * PAD, width), jnp.float32), plane, plane, plane],
        compiler_params=pltpu.CompilerParams(vmem_limit_bytes=24 * 2**20),
        cost_estimate=pl.CostEstimate(flops=16 * length * width * 256, bytes_accessed=8 * 2**20, transcendentals=8 * length * width),
        name="recurrence",
    )(before, taps, rates, recall_maps, admit_maps)


def contract_last(left, right):
    return lax.dot_general(
        left, right, (((1,), (1,)), ((), ())), preferred_element_type=jnp.float32
    )


def gather(shard):
    copies = lax.axis_size("rep")
    if shard.shape[0] % (16 * copies):
        return lax.all_gather(shard.astype(jnp.bfloat16), "fs", axis=0, tiled=True)
    rows = shard.shape[0] // copies
    part = lax.dynamic_slice_in_dim(shard, lax.axis_index("rep") * rows, rows, 0)
    return lax.all_gather(part.astype(jnp.bfloat16), ("fs", "rep"), axis=0, tiled=True)


def body(
    tokens,
    first_gain,
    in_matrix,
    in_scale,
    conv_taps,
    decay_rate,
    recall_maps,
    admit_maps,
    out_matrix,
    out_scale,
    second_gain,
    up_matrix,
    up_scale,
    down_matrix,
    down_scale,
):
    stream = tokens.reshape(tokens.shape[1], tokens.shape[2]).astype(jnp.float32)
    factors = lax.all_gather(
        jnp.stack([out_scale, down_scale]).astype(jnp.bfloat16), "fs", axis=1, tiled=True
    )
    in_cols = gather(in_matrix)
    normed = normalize(stream, first_gain).astype(jnp.bfloat16)
    before = (
        jnp.dot(normed, in_cols, preferred_element_type=jnp.float32) * in_scale.astype(jnp.bfloat16)
    ).astype(jnp.bfloat16)
    mixed = recurrence(before, conv_taps, decay_rate, recall_maps, admit_maps)
    partial_value = contract_last(mixed, gather(out_matrix))
    middle = stream + factors[0] * lax.psum(partial_value.astype(jnp.bfloat16), "tp").astype(
        jnp.float32
    )
    second_normed = normalize(middle, second_gain).astype(jnp.bfloat16)
    raised = jnp.dot(second_normed, gather(up_matrix), preferred_element_type=jnp.float32)
    active = jnp.square(jax.nn.relu(raised * up_scale.astype(jnp.bfloat16))).astype(jnp.bfloat16)
    lowered = contract_last(active, gather(down_matrix))
    result = (
        middle + factors[1] * lax.psum(lowered.astype(jnp.bfloat16), "tp").astype(jnp.float32)
    ).astype(jnp.bfloat16)
    return result.reshape(tokens.shape)

MESH = pl.DeviceIdType.MESH
UNITS = 22
SPLIT = 2
OWN_TO_MATE = (2, 3, 4, 5, 6, 7, 8, 9, 10, 11, 12, 13, 14, 15, 16)
OWN_TO_MATE_AFTER = {10: (17,), 17: (18, 19, 20, 21)}
OWN_TO_OTHER = (0, 1)
OWN_TO_OTHER_AFTER = {1: (2, 3, 4, 5), 5: (6, 7), 7: (8,), 8: (9, 10), 10: (11, 12, 13), 12: (14, 15), 14: (16,), 16: (17, 18, 19), 17: (20,), 18: (21,)}
EDGE_SENDS = ((1, 2), (1, 3), (1, 4), (1, 5), (0, 2), (0, 3), (0, 4), (0, 5), (1, 6), (1, 7), (1, 8), (1, 9), (1, 10), (1, 11), (1, 12), (1, 13), (0, 6), (0, 7), (0, 8), (0, 9), (0, 10), (0, 11), (0, 12), (0, 13), (1, 14), (1, 15), (1, 16), (1, 17), (1, 18), (1, 19), (1, 20), (1, 21), (0, 14), (0, 15), (0, 16), (0, 17), (0, 18), (0, 19), (0, 20), (0, 21))
DOWN_ORDER = ((0, 0), (0, 1), None, (1, 0), (1, 1), (0, 2), (1, 2), (0, 3), (1, 3), (0, 4), (1, 4), (0, 5), (1, 5), (0, 6), (1, 6), (0, 7), (1, 7))
LAG = 4
EDGE_SERVES = (
    (2, 3, 4, 5, 6, 7, 8, 9, 10, 11, 12, 13, 14, 15, 16, 24, 25, 26, 27, 46, 47),
    (48,),
    (),
    (49,),
    (28,),
    (29,),
    (),
    (50,),
    (),
    (51,),
    (),
    (30,),
    (),
    (),
    (),
    (),
    (52,),
    (),
    (),
    (31,),
    (),
    (),
    (32, 53),
    (),
    (),
    (54,),
    (17,),
    (33,),
    (34,),
    (35,),
    (55,),
    (56,),
    (36,),
    (),
    (37,),
    (),
    (57, 58, 38, 59),
    (),
    (),
    (),
    (),
    (),
    (),
    (),
    (),
    (),
    (60, 39),
    (40, 41),
    (),
    (),
    (),
    (),
    (),
    (),
    (61,),
    (),
    (18,),
    (),
    (),
    (),
    (19,),
    (),
    (),
    (),
    (20,),
    (),
    (21,),
    (),
    (),
    (42,),
    (),
    (62,),
    (43,),
    (),
    (),
    (),
    (63,),
    (64, 65),
    (),
    (),
    (),
    (),
    (),
    (),
    (),
    (),
    (),
    (),
    (),
    (),
    (),
    (),
    (),
)
INNER_SERVES = (
    (),
    (),
    (),
    (),
    (0, 22, 1, 23),
    (44, 45),
    (24,),
    (25, 26),
    (),
    (),
    (27, 2),
    (3, 4, 46),
    (5,),
    (47,),
    (),
    (48,),
    (),
    (49,),
    (28,),
    (29,),
    (6,),
    (7,),
    (),
    (8,),
    (50, 9),
    (),
    (),
    (51, 10),
    (),
    (),
    (),
    (),
    (30, 11),
    (),
    (),
    (52, 12),
    (),
    (),
    (31, 13, 32),
    (),
    (),
    (53,),
    (54,),
    (33,),
    (34,),
    (35,),
    (55,),
    (56,),
    (36, 14, 37, 15),
    (),
    (),
    (),
    (57, 16, 58, 17, 38, 18, 59, 19),
    (),
    (),
    (),
    (),
    (),
    (),
    (),
    (),
    (60, 20),
    (39, 21),
    (40, 41),
    (),
    (),
    (),
    (),
    (),
    (61,),
    (),
    (),
    (42,),
    (),
    (),
    (),
    (62,),
    (43,),
    (),
    (),
    (63,),
    (),
    (64,),
    (),
    (),
    (65,),
    (),
    (),
    (),
    (),
    (),
    (),
    (),
    (),
    (),
    (),
    (),
    (),
    (),
    (),
    (),
    (),
    (),
    (),
    (),
    (),
    (),
    (),
    (),
)


def layer_kernel(
    names, tokens_hbm, first_hbm, in_hbm, in_scale_hbm, taps_hbm, rate_hbm, recall_hbm, admit_hbm,
    out_hbm, out_scale_hbm, second_hbm, up_hbm, up_scale_hbm, down_hbm, down_scale_hbm,
    result_ref,
    first_ref, in_scale_ref, taps_ref, rate_ref, second_ref, up_scale_ref, tokens, in_own, out_own, up_own, down_own, recall_ref, admit_ref,
    in_all, out_all, up_all, down_all, scales_all, normed, guest, before, second_normed, padded, decay, drive, prefix,
    mixed, active, parts, near_parts, pairs, far_pairs, middle, load, send, recv,
):
    replica, place, rank = (lax.axis_index(name) for name in names)
    rep_name, fs_name, tp_name = names
    fs = 4
    length, model = tokens.shape
    block = model // fs
    half, quarter = block // 2, block // 4
    mate = place + 1 - 2 * lax.rem(place, 2)
    inner = lax.rem(lax.div(place + 1, 2), 2)
    other = fs - 1 - place
    other_mate = fs - 1 - mate
    slots = (mate, inner * other + (1 - inner) * other_mate, inner * other_mate + (1 - inner) * other)
    core = lax.rem(rank, 2)
    near = rank + 1 - 2 * core
    far = lax.rem(rank + 2, 4)
    recvs, groups = [0], {}

    def fresh():
        recvs[0] += 1
        return recvs[0] - 1

    def whole_copy(src, dst, axis, peer, group, into):
        return pltpu.make_async_remote_copy(
            src_ref=src, dst_ref=dst, send_sem=send.at[groups.setdefault(group, len(groups))], recv_sem=recv.at[into],
            device_id={axis: peer}, device_id_type=MESH,
        )

    def bytes_of(ref):
        return math.prod(ref.shape) * jnp.dtype(ref.dtype).itemsize

    def waiter(size, group, into):
        count = size // bytes_of(up_all.at[0])
        return whole_copy(up_all.at[0:count, :], up_all.at[0:count, :], tp_name, near, group, into)

    class copy:
        def __init__(self, src, dst, axis, peer, group, into=None):
            self.into = fresh() if into is None else into
            self.group, self.size = group, bytes_of(src)
            self.one = whole_copy(src, dst, axis, peer, group, self.into)
            self.start, self.wait_recv, self.wait_send = self.one.start, self.one.wait_recv, self.one.wait_send

    common_sent, edge_sent, inner_sent = {}, {}, {}

    def start(one, sent=common_sent):
        one.start()
        sent.setdefault(one.group, []).append(one)

    def drain(sent):
        for group, copies in sent.items():
            if len(copies) == 1:
                copies[0].wait_send()
            else:
                waiter(sum(one.size for one in copies), group, copies[0].into).wait_send()

    def wait_all(copies):
        waiter(sum(one.size for one in copies), copies[0].group, copies[0].into).wait_recv()

    barrier = pltpu.get_barrier_semaphore()
    greeted = [(rep_name, 1 - replica)]
    greeted += [(fs_name, mate), (tp_name, near), (tp_name, far)]

    def greet(axis, peer):
        pl.semaphore_signal(barrier, inc=1, device_id={axis: peer}, device_id_type=MESH)

    for axis, peer in greeted:
        greet(axis, peer)
    pl.when(inner == 1)(lambda: greet(fs_name, other))

    loads = [
        pltpu.make_async_copy(src, dst, load.at[i])
        for i, (src, dst) in enumerate((
            (in_hbm, in_own), (out_hbm, out_own), (first_hbm, first_ref), (tokens_hbm, tokens), (up_hbm, up_own),
            (down_hbm, down_own), (out_scale_hbm, scales_all.at[place, 0:1, :]), (down_scale_hbm, scales_all.at[place, 1:2, :]),
            (in_scale_hbm, in_scale_ref), (taps_hbm, taps_ref), (rate_hbm, rate_ref), (second_hbm, second_ref),
            (up_scale_hbm, up_scale_ref), (recall_hbm, recall_ref), (admit_hbm, admit_ref),
        ))
    ]
    for one in loads:
        one.start()
    load_in, load_out, load_first, load_tokens, load_up, load_down = loads[:6]
    load_scales, load_rest = loads[6:8], loads[8:]

    own_rows = pl.ds(pl.multiple_of(place * block, block), block)
    load_in.wait()
    in_all[own_rows, :] = in_own[...].astype(jnp.bfloat16)
    load_out.wait()
    out_all[own_rows, :] = out_own[...].astype(jnp.bfloat16)

    wide = up_all.shape[1] // 2

    def view(owner, unit, side):
        def rows(first, count):
            return pl.ds(pl.multiple_of(owner * block + side * half + first, count), count)

        def columns(part):
            return slice(part * wide, (part + 1) * wide)

        eighth = quarter // 2
        if unit < 2:
            return in_all.at[rows(unit * quarter, quarter), :]
        if unit < 6:
            return out_all.at[rows((unit - 2) * eighth, eighth), :]
        if unit < 14:
            return up_all.at[rows((unit - 6) % 4 * eighth, eighth), columns((unit - 6) // 4)]
        return down_all.at[rows((unit - 14) // 4 * quarter + unit % 2 * eighth, eighth), columns((unit - 14) % 4 // 2)]

    to_mate, extra, to_other, pass_mate, pass_other, pass_last, swaps = [], [], [], [], [], [], []
    bundles = [(0, 1)] + [tuple(range(i, i + 4)) for i in range(2, UNITS, 4)]
    landings = {}
    for bundle in bundles:
        shared = [fresh() for _ in range(3 if bundle[0] >= 14 else 1)] * (1 if bundle[0] >= 14 else 3)
        for unit in bundle:
            landings[unit] = shared
    for unit in range(UNITS):
        into = [fresh() for _ in range(3)]
        own, first, second, third = (view(owner, unit, replica) for owner in (place,) + slots)
        rest = view(place, unit, 1 - replica)
        land = landings[unit]
        to_mate.append(copy(own, own, fs_name, mate, "to_mate", into[0]))
        extra.append(copy(rest, rest, fs_name, mate, "extra", land[0]) if unit >= SPLIT else None)
        to_other.append(copy(own, own, fs_name, other, "to_other", into[1]))
        pass_mate.append(copy(first, first, fs_name, other, "pass_mate", into[2]))
        pass_other.append(copy(second, second, fs_name, mate, "pass_other", into[1]) if unit >= SPLIT else None)
        pass_last.append(copy(third, third, fs_name, mate, "pass_last", into[2]))
        swaps.append([copy(part, part, rep_name, 1 - replica, f"swap{j}", land[j]) for j, part in enumerate((first, second, third))])
    arrivals = (to_mate, to_other, pass_last)

    def serve_edge(codes):
        for code in codes:
            slot, unit = code // UNITS, code % UNITS
            arrivals[slot][unit].wait_recv()
            start(swaps[unit][slot], edge_sent)

    def serve_inner(codes):
        for code in codes:
            slot, unit = code // UNITS, code % UNITS
            arrivals[slot][unit].wait_recv()
            if slot or unit < SPLIT:
                start(swaps[unit][slot], inner_sent)
            if slot == 0:
                start(pass_mate[unit], inner_sent)
                for u in OWN_TO_OTHER_AFTER.get(unit, ()):
                    start(to_other[u], inner_sent)
            elif unit >= SPLIT:
                start((pass_other, pass_last)[slot - 1][unit], inner_sent)
            if slot == 2:
                for u in OWN_TO_MATE_AFTER.get(unit, ()):
                    start(to_mate[u], inner_sent)

    points = {"edge": 0, "inner": 0}

    def edge_next():
        points["edge"] += 1
        return EDGE_SERVES[points["edge"] - 1]

    def inner_next():
        points["inner"] += 1
        return INNER_SERVES[points["inner"] - 1]

    def serve():
        edge_codes, inner_codes = edge_next(), inner_next()
        if edge_codes:
            pl.when(inner == 0)(lambda: serve_edge(edge_codes))
        if inner_codes:
            pl.when(inner == 1)(lambda: serve_inner(inner_codes))

    def landed(units, taken=(0, 1, 2)):
        wait_all([swaps[unit][slot] for unit in units for slot in taken])

    piece = 32
    pieces = length // 4 // piece

    def guest_rows(owner, i):
        return pl.ds(pl.multiple_of(owner * (length // 4) + i * piece, piece), piece)

    tok, tok_far, tok_near, tok_onward = [], [], [], []
    guest_near = fresh()
    for i in range(pieces):
        mine, theirs = guest_rows(rank, i), guest_rows(far, i)
        tok.append(copy(normed.at[mine, :], guest.at[mine, :], fs_name, mate, "guest"))
        tok_far.append(copy(guest.at[mine, :], guest.at[mine, :], tp_name, far, "guest"))
        tok_near.append(copy(guest.at[mine, :], guest.at[mine, :], tp_name, near, "guest", guest_near))
        tok_onward.append(copy(guest.at[theirs, :], guest.at[theirs, :], tp_name, near, "guest", guest_near))
    step = 256
    tiles = [slice(i * step, (i + 1) * step) for i in range(in_all.shape[1] // step)]
    given_before = [copy(before.at[:, at], before.at[:, at], fs_name, mate, "guest") for at in tiles]

    pl.when(inner == 0)(lambda: pl.semaphore_wait(barrier, len(greeted)))
    pl.when(inner == 1)(lambda: pl.semaphore_wait(barrier, len(greeted) + 1))

    @pl.when(inner == 0)
    def _():
        for unit in range(SPLIT):
            start(to_mate[unit], edge_sent)

    @pl.when(inner == 1)
    def _():
        for unit in OWN_TO_OTHER:
            start(to_other[unit], inner_sent)
        for unit in OWN_TO_MATE:
            if unit < 6:
                start(to_mate[unit], inner_sent)

    def norm_rows(at):
        normed[at, :] = normalize(tokens[at, :].astype(jnp.float32), first_ref[...]).astype(jnp.bfloat16)

    load_first.wait()
    load_tokens.wait()

    @pl.when(inner == 0)
    def _():
        for i in range(pieces):
            norm_rows(guest_rows(rank, i))
            start(tok[i], edge_sent)

    load_up.wait()
    up_all[own_rows, :] = up_own[...].astype(jnp.bfloat16)
    load_down.wait()
    down_all[own_rows, :] = down_own[...].astype(jnp.bfloat16)
    for one in load_scales:
        one.wait()
    into = [fresh() for _ in range(3)]
    own, first, second, third = (scales_all.at[owner] for owner in (place,) + slots)
    scale_in = [
        copy(own, own, fs_name, mate, "scale0", into[0]), copy(own, own, fs_name, other, "scale1", into[1]),
        copy(third, third, fs_name, mate, "scale2", into[2]),
    ]
    scale_out = [
        copy(first, first, fs_name, other, "scale3", into[2]), copy(second, second, fs_name, mate, "scale4", into[1]), scale_in[2],
    ]
    start(scale_in[0])
    pl.when(inner == 1)(lambda: start(scale_in[1], inner_sent))

    def pass_scales(slot):
        scale_in[slot].wait_recv()
        start(scale_out[slot], inner_sent)

    for one in load_rest:
        one.wait()
    edge = jnp.zeros((PAD, padded.shape[1]), jnp.float32)
    padded[pl.ds(0, PAD), :] = edge
    padded[pl.ds(PAD + length, PAD), :] = edge

    @pl.when(inner == 0)
    def _():
        for whole, unit in EDGE_SENDS:
            start((to_mate if whole else extra)[unit], edge_sent)
        serve_edge(edge_next())
        for one, at in zip(given_before, tiles):
            one.wait_recv()
            padded[pl.ds(PAD, length), at] = before[:, at].astype(jnp.float32)

    @pl.when(inner == 1)
    def _():
        for unit in OWN_TO_MATE:
            if unit >= 6:
                start(to_mate[unit], inner_sent)
        tile = 64
        for i in range(4):

            def norm_step(k, _, i=i):
                norm_rows(pl.ds(pl.multiple_of((2 * i + k) * tile, tile), tile))
                return 0

            lax.fori_loop(0, length // tile // 4, norm_step, 0)
            serve_inner(inner_next())
        for i in range(pieces):
            serve_inner(inner_next())
            tok[i].wait_recv()
            start(tok_far[i], inner_sent)
            start(tok_near[i], inner_sent)
        pass_scales(0)
        pass_scales(1)
        for i in range(pieces):
            serve_inner(inner_next())
            tok_far[i].wait_recv()
            start(tok_onward[i], inner_sent)
        serve_inner(inner_next())
        landed(range(SPLIT))
        wait_all(tok_near + tok_onward)

        def project_in(values, at):
            product = jnp.dot(values[...], in_all[:, at], preferred_element_type=jnp.float32)
            return (product * in_scale_ref[:, at].astype(jnp.bfloat16).astype(jnp.float32)).astype(jnp.bfloat16)

        for one, at in zip(given_before, tiles):
            before[:, at] = project_in(guest, at)
            start(one, inner_sent)
            serve_inner(inner_next())
        pass_scales(2)
        for at in tiles:
            padded[pl.ds(PAD, length), at] = project_in(normed, at).astype(jnp.float32)
            serve_inner(inner_next())

    gate_part(padded, taps_ref, rate_ref, recall_ref, admit_ref, decay, drive, length, serve)
    scan_part(decay, drive, prefix, mixed, length, serve)

    serve()
    landed(bundles[1])

    @pl.when(inner == 0)
    def _():
        for one in scale_in:
            one.wait_recv()

    chunks = model // step
    rows = length // 2
    batch = rows // 2
    kept = pl.ds(pl.multiple_of(core * rows, rows), rows)
    given = pl.ds(pl.multiple_of((1 - core) * rows, rows), rows)

    def of_batch(h):
        return slice(h * batch, (h + 1) * batch)

    def factor(owner, which, at):
        return scales_all[owner, which : which + 1, at].astype(jnp.bfloat16).astype(jnp.float32)

    to_near = [copy(parts.at[0, k, given, :], near_parts.at[0, k], tp_name, near, "reduce") for k in range(chunks)]
    to_far = [
        [
            [copy(pairs.at[stage, k, of_batch(h), :], far_pairs.at[stage, k, of_batch(h), :], tp_name, far, "reduce") for k in range(chunks)]
            for h in range(2)
        ]
        for stage in range(2)
    ]

    def far_total(stage, h, k):
        to_far[stage][h][k].wait_recv()
        return pairs[stage, k, of_batch(h), :].astype(jnp.float32) + far_pairs[stage, k, of_batch(h), :].astype(jnp.float32)

    for k in range(chunks + 2):
        if k < chunks:
            product = contract_last(mixed[...], out_all[k * step : (k + 1) * step, :])
            parts[0, k] = product.astype(jnp.bfloat16)
            start(to_near[k])
        serve()
        if k >= 2:
            to_near[k - 2].wait_recv()
            total = parts[0, k - 2, kept, :].astype(jnp.float32) + near_parts[0, k - 2].astype(jnp.float32)
            pairs[0, k - 2] = total.astype(jnp.bfloat16)
            start(to_far[0][0][k - 2])
    for k in range(chunks):
        start(to_far[0][1][k])

    spreads = []

    def middle_rows(h):
        squares = jnp.zeros((batch, 1), jnp.float32)
        at_rows = pl.ds(pl.multiple_of(core * rows + h * batch, batch), batch)
        for k in range(chunks):
            serve()
            at = slice(k * step, (k + 1) * step)
            inside = slice(k * step % block, k * step % block + step)
            value = tokens[at_rows, at].astype(jnp.float32) + factor(k * step // block, 0, inside) * far_total(0, h, k)
            middle[of_batch(h), at] = value
            squares = squares + jnp.sum(value * value, axis=1, keepdims=True)
        inverse = lax.rsqrt(squares * (1.0 / model) + EPSILON)
        at = pl.ds(pl.multiple_of(h * rows + core * batch, batch), batch)
        second_normed[at, :] = (middle[of_batch(h), :] * inverse * second_ref[...]).astype(jnp.bfloat16)
        spreads.append(copy(second_normed.at[at, :], second_normed.at[at, :], tp_name, near, "spread"))
        start(spreads[h])

    def up_rows(h):
        serve()
        spreads[h].wait_recv()
        at_rows = slice(h * rows, (h + 1) * rows)
        for part in range(2):
            serve()
            if h == 0:
                landed(bundles[2 + part])
            for i in range(part * (wide // step), (part + 1) * (wide // step)):
                at = slice(i * step, (i + 1) * step)
                raised = jnp.dot(second_normed[at_rows, :], up_all[:, at], preferred_element_type=jnp.float32)
                raised = raised * up_scale_ref[:, at].astype(jnp.bfloat16).astype(jnp.float32)
                active[at_rows, at] = jnp.square(jnp.maximum(raised, 0.0)).astype(jnp.bfloat16)
                serve()

    middle_rows(0)
    up_rows(0)
    middle_rows(1)

    owners = [(place, 0, None), (place, 1, None)] + [(slots[j], q, j) for q in range(2) for j in range(3)]
    turns = [turn for turn in DOWN_ORDER if turn is not None]
    down_near, finals, final = [], [], fresh()

    def pair_down(n):
        h, k = turns[n]
        serve()
        down_near[n].wait_recv()
        at = pl.ds(pl.multiple_of(h * rows + core * batch, batch), batch)
        total = parts[1, k, at, :].astype(jnp.float32) + near_parts[1, k, of_batch(h), :].astype(jnp.float32)
        pairs[1, k, of_batch(h), :] = total.astype(jnp.bfloat16)
        start(to_far[1][h][k])

    def finish(n):
        h, k = turns[n]
        owner, q, _ = owners[k]
        serve()
        total = far_total(1, h, k)
        at_rows = pl.ds(pl.multiple_of(core * rows + h * batch, batch), batch)
        for s in range(2):
            inside = slice(s * half + q * quarter, s * half + (q + 1) * quarter)
            at = pl.ds(pl.multiple_of(owner * block + s * half + q * quarter, quarter), quarter)
            value = middle[of_batch(h), at] + factor(owner, 1, inside) * total[:, s * quarter : (s + 1) * quarter]
            result_ref[at_rows, at] = value.astype(jnp.bfloat16)
            finals.append(copy(result_ref.at[at_rows, at], result_ref.at[at_rows, at], tp_name, near, "spread", final))
            start(finals[-1])

    n = 0
    for turn in DOWN_ORDER:
        if turn is None:
            up_rows(1)
            continue
        h, k = turn
        owner, q, j = owners[k]
        if j is not None and h == 0:
            serve()
            landed(bundles[4 + q], (j,))
        matrix = [
            down_all[pl.ds(pl.multiple_of(owner * block + s * half + q * quarter, quarter), quarter), :] for s in range(2)
        ]
        product = contract_last(active[h * rows : (h + 1) * rows, :], jnp.concatenate(matrix, axis=0))
        parts[1, k, h * rows : (h + 1) * rows, :] = product.astype(jnp.bfloat16)
        away = pl.ds(pl.multiple_of(h * rows + (1 - core) * batch, batch), batch)
        down_near.append(copy(parts.at[1, k, away, :], near_parts.at[1, k, of_batch(h), :], tp_name, near, "reduce"))
        start(down_near[n])
        if n >= 1:
            pair_down(n - 1)
        if n >= LAG:
            finish(n - LAG)
        n += 1
    pair_down(n - 1)
    for m in range(n - LAG, n):
        finish(m)
    serve()
    wait_all(finals)
    drain(common_sent)
    pl.when(inner == 0)(lambda: drain(edge_sent))
    pl.when(inner == 1)(lambda: drain(inner_sent))


def fused_body(
    tokens, first_gain, in_matrix, in_scale, conv_taps, decay_rate, recall_maps, admit_maps,
    out_matrix, out_scale, second_gain, up_matrix, up_scale, down_matrix, down_scale,
):
    length, model = tokens.shape[1:]
    width, hidden = in_matrix.shape[1], up_matrix.shape[1]
    fs = lax.axis_size("fs")
    block, step = model // fs, 256
    directions = decay_rate.shape[0]
    plane = pltpu.VMEM((directions, width // LANES, SEGMENTS * (length // SEGMENTS + GAP), LANES), jnp.float32)
    gate = pltpu.VMEM(recall_maps.shape, jnp.float32)
    pieces = pltpu.VMEM((2, model // step, length // 2, step), jnp.bfloat16)
    rows = pltpu.VMEM((length, model), jnp.bfloat16)
    channels = pltpu.VMEM((length, width), jnp.bfloat16)
    vmem, hbm = pl.BlockSpec(memory_space=pltpu.VMEM), pl.BlockSpec(memory_space=pl.ANY)
    arrived = UNITS * 3 + 27 + 7 * (model // step)
    result = pl.pallas_call(
        functools.partial(layer_kernel, ("rep", "fs", "tp")),
        out_shape=pltpu.VMEM((length, model), jnp.bfloat16),
        in_specs=[hbm] * 15,
        out_specs=vmem,
        scratch_shapes=[
            pltpu.VMEM((1, model), jnp.float32),
            pltpu.VMEM((1, width), jnp.float32),
            pltpu.VMEM(conv_taps.shape, jnp.float32),
            pltpu.VMEM(decay_rate.shape, jnp.float32),
            pltpu.VMEM((1, model), jnp.float32),
            pltpu.VMEM((1, hidden), jnp.float32),
            rows,
            pltpu.VMEM((block, width), jnp.float32),
            pltpu.VMEM((block, width), jnp.float32),
            pltpu.VMEM((block, hidden), jnp.float32),
            pltpu.VMEM((block, hidden), jnp.float32),
            gate, gate,
            pltpu.VMEM((model, width), jnp.bfloat16),
            pltpu.VMEM((model, width), jnp.bfloat16),
            pltpu.VMEM((model, hidden), jnp.bfloat16),
            pltpu.VMEM((model, hidden), jnp.bfloat16),
            pltpu.VMEM((fs, 2, block), jnp.float32),
            rows, rows, channels, rows,
            pltpu.VMEM((length + 2 * PAD, width), jnp.float32),
            plane, plane, plane,
            channels,
            pltpu.VMEM((length, hidden), jnp.bfloat16),
            pltpu.VMEM((2, model // step, length, step), jnp.bfloat16),
            pieces, pieces, pieces,
            pltpu.VMEM((length // 2, model), jnp.float32),
            pltpu.SemaphoreType.DMA((15,)),
            pltpu.SemaphoreType.DMA((17,)),
            pltpu.SemaphoreType.DMA((arrived,)),
        ],
        compiler_params=pltpu.CompilerParams(
            collective_id=0, has_side_effects=True, vmem_limit_bytes=59 * 2**20
        ),
        name="layer",
    )(
        tokens.reshape(length, model), first_gain[None], in_matrix, in_scale[None], conv_taps, decay_rate,
        recall_maps, admit_maps, out_matrix, out_scale[None], second_gain[None], up_matrix, up_scale[None], down_matrix,
        down_scale[None],
    )
    return result.reshape(tokens.shape)


def solution(mesh):
    placed = (
        P(("rep", "fs"), None, None),
        P(),
        P("fs", "tp"),
        P("tp"),
        P(None, "tp"),
        P(None, "tp"),
        P(None, "tp", None, None),
        P(None, "tp", None, None),
        P("fs", "tp"),
        P("fs"),
        P(),
        P("fs", "tp"),
        P("tp"),
        P("fs", "tp"),
        P("fs"),
    )
    small = (mesh.shape["rep"], mesh.shape["fs"], mesh.shape["tp"]) == (2, 4, 4)
    return jax.shard_map(
        fused_body if small else body, mesh=mesh, in_specs=placed, out_specs=P(("rep", "fs"), None, None), check_vma=False
    )
```
